128 devices in a mesh: sp: 32 (over y, x, core), tp: 4 (over z).
Axes of the slice: x: 4, y: 4, z: 4, core: 2. Of those that a mesh axis runs over, the one named last changes fastest.
Arguments:
- block_input: bfloat16 [4096, 1024], P('sp'), may hold values from -6 to 6
- w_query: bfloat16 [1024, 1024], P(None, 'tp'), may hold values from -0.1875 to 0.1875
- w_forget_fwd: bfloat16 [1024, 1024], P(None, 'tp'), may hold values from -0.1875 to 0.1875
- w_forget_bwd: bfloat16 [1024, 1024], P(None, 'tp'), may hold values from -0.1875 to 0.1875
- w_value: bfloat16 [1024, 1024], P(None, 'tp'), may hold values from -0.1875 to 0.1875
- floor_rate: float32 [2, 1024], P(None, 'tp'), may hold values from 0.2 to 6
- gain: float32 [128], replicated, may hold values from 0.1 to 1.9
- cotangent: bfloat16 [4096, 1024], P('sp', 'tp'), may hold values from -6 to 6
Outputs:
- grad_input: bfloat16 [4096, 1024], P(('sp', 'tp'))
- grad_query_weight: float32 [1024, 1024], P('sp', 'tp')
- grad_floor: float32 [2, 1024], P(None, 'tp')
The draws below stay inside these ranges and needn't reach their ends.
All inputs are finite; a program needn't handle non-finite values.
Results may differ from the reference program's by a relative error of at most 0.0045.
Values sent between devices are 32-bit elements.
A program may use at most 64 MiB of HBM per device.

```python
import math
import jax
import jax.numpy as jnp
from jax import lax

HEADS = 8
KDIM = 128
VDIM = 128
D = 1024
TOK_DEV = 128
TOKENS = 4096


def with_spikes(result, rng, source, target, parts, factor):
    owner, partner = [(jnp.arange(result.shape[position]) // (result.shape[position] // parts)).reshape([-1 if axis == position else 1 for axis in range(result.ndim)]) for position in (source, target)]
    chosen = jax.random.permutation(rng, parts)[partner]
    strong = (owner == chosen) | (owner == (partner + parts // 2) % parts)
    return jnp.where(strong, factor * result, result)


def steps_of(own_key, dims, cuts, smallest, high):
    level = 1.0
    for position, blocks in cuts:
        steps = jax.random.uniform(jax.random.fold_in(jax.random.fold_in(own_key, 6), position), (blocks,), jnp.float32, smallest / len(cuts), high / len(cuts))
        level = level * jnp.repeat(jnp.exp(steps), dims[position] // blocks).reshape((-1,) + (1,) * (len(dims) - 1 - position))
    return level


def noise(rng, dims, scale, bound, cuts=(), dtype=jnp.bfloat16):
    level = steps_of(rng, dims, cuts, -0.22, 0.18) if cuts else 1.0
    array = jax.random.normal(rng, dims, jnp.float32) * scale * level
    return jnp.minimum(jnp.maximum(array, -bound), bound).astype(dtype)


def heavy_noise(key, shape, width, limit, split, heavy, kind=jnp.bfloat16):
    entries = width * jax.random.normal(key, shape, jnp.float32)
    if split:
        entries = entries * steps_of(key, shape, split, -0.22, 0.18)
    return jnp.clip(with_spikes(entries, jax.random.fold_in(key, 3), *heavy), -limit, limit).astype(kind)


def setup_inputs(seed: int = 0) -> dict:
    streams_of = jax.random.split(jax.random.key(seed), 9)
    return {
        "block_input": heavy_noise(streams_of[0], (TOKENS, D), 1.0, 6.0, ((0, 32),), (0, 1, 32, 2.75)),
        "w_query": noise(streams_of[1], (D, HEADS * KDIM), D ** -0.5, 0.1875, ((1, 4),)),
        "w_forget_fwd": noise(streams_of[2], (D, HEADS * KDIM), D ** -0.5, 0.1875, ((1, 4),)),
        "w_forget_bwd": noise(streams_of[3], (D, HEADS * KDIM), D ** -0.5, 0.1875, ((1, 4),)),
        "w_value": noise(streams_of[4], (D, HEADS * VDIM), D ** -0.5, 0.1875, ((1, 4),)),
        "floor_rate": jnp.clip(jnp.exp(math.log(6.0) - 3.4011974 * jax.random.uniform(streams_of[5], (2, HEADS * KDIM), jnp.float32) ** steps_of(streams_of[5], (2, HEADS * KDIM), ((1, 4),), -0.2, 0.2)), 0.2, 6.0),
        "gain": jnp.clip(1.0 + 0.18 * jax.random.normal(streams_of[6], (VDIM,), jnp.float32), 0.1, 1.9),
        "cotangent": noise(streams_of[7], (TOKENS, HEADS * VDIM), 1.0, 6.0, ((0, 32), (1, 4))),
    }


FINEST_ROUNDING = lax.Precision.HIGHEST
NORM_EPS = 1e-06

def gate_maps(raw_gate, floor_rates, seq_total):
    step_rate = floor_rates / seq_total
    opening = -jnp.expm1(-step_rate)
    log_forget = jnp.logaddexp(-step_rate, jnp.log(opening) + jax.nn.log_sigmoid(raw_gate))
    return (opening * jax.nn.sigmoid(-raw_gate), log_forget)

def span_output(queries, key_gate, log_forget, payload_entries, arriving_signal):
    cumul = jnp.cumsum(log_forget, axis=0)
    faded_asking_vector = queries * jnp.exp(cumul)
    k_dec = key_gate * jnp.exp(-cumul)
    tok_count = queries.shape[0]
    scores = jnp.einsum('thk,shk->hts', faded_asking_vector, k_dec, precision=FINEST_ROUNDING)
    scores = scores * jnp.tril(jnp.ones((tok_count, tok_count), jnp.float32))
    inner_part = jnp.einsum('hts,shv->thv', scores, payload_entries, precision=FINEST_ROUNDING)
    external_portion = jnp.einsum('nea,eaw->new', faded_asking_vector, arriving_signal, precision=FINEST_ROUNDING)
    return inner_part + external_portion

def span_carry(key_gate, log_forget, payload_entries):
    cumul = jnp.cumsum(log_forget, axis=0)
    final_running_total = cumul[-1]
    scaled_by_factor = key_gate * jnp.exp(final_running_total[None] - cumul)
    return (jnp.exp(final_running_total), jnp.einsum('xzp,xzo->zpo', scaled_by_factor, payload_entries, precision=FINEST_ROUNDING))

def normed(mixed, gain):
    mean_square = lax.optimization_barrier(jnp.mean(mixed * mixed, axis=-1, keepdims=True))
    return mixed * lax.rsqrt(mean_square + NORM_EPS) * gain

def run_direction(queries, key_gate, log_forget, payload_entries):
    seq_total, head_count, key_dim = queries.shape
    val_dim = payload_entries.shape[2]
    block_count = seq_total // TOK_DEV

    def blocks(source):
        return source.reshape((block_count, TOK_DEV) + source.shape[1:])

    def advance(carried, inputs):
        q_blk, k_blk, f_blk, v_blk = inputs
        mixed = span_output(q_blk, k_blk, f_blk, v_blk, carried)
        keep_all, local_sum = span_carry(k_blk, f_blk, v_blk)
        return (keep_all[..., None] * carried + local_sum, mixed)
    zero_state = jnp.zeros((head_count, key_dim, val_dim), jnp.float32)
    _, mixed_all = lax.scan(advance, zero_state, (blocks(queries), blocks(key_gate), blocks(log_forget), blocks(payload_entries)))
    return mixed_all.reshape(seq_total, head_count, val_dim)

def reference(block_input, w_query, w_forget_fwd, w_forget_bwd, w_value, floor_rate, gain, cotangent):
    seq_total = block_input.shape[0]

    def project(weight, per_head):
        pre = jnp.dot(block_input, weight, preferred_element_type=jnp.float32).astype(jnp.bfloat16)
        return lax.optimization_barrier(pre).astype(jnp.float32).reshape(seq_total, HEADS, per_head)
    raw_query = project(w_query, KDIM)
    raw_value = project(w_value, VDIM)
    raw_fwd = project(w_forget_fwd, KDIM)
    raw_bwd = project(w_forget_bwd, KDIM)
    floor_rates = floor_rate.reshape(2, HEADS, KDIM)

    def mixer(query_in, value_in, gate_fwd, gate_bwd, rate_pair):
        scaled = query_in * KDIM ** (-0.5)
        key_fwd, logf_fwd = gate_maps(gate_fwd, rate_pair[0], float(seq_total))
        key_bwd, logf_bwd = gate_maps(gate_bwd, rate_pair[1], float(seq_total))
        out_fwd = run_direction(scaled, key_fwd, logf_fwd, value_in)
        out_bwd = run_direction(jnp.flip(scaled, 0), jnp.flip(key_bwd, 0), jnp.flip(logf_bwd, 0), jnp.flip(value_in, 0))
        return normed(out_fwd + jnp.flip(out_bwd, 0), gain)
    _, mixer_back = jax.vjp(mixer, raw_query, raw_value, raw_fwd, raw_bwd, floor_rates)
    d_query, d_value, d_fwd, d_bwd, d_rates = mixer_back(cotangent.astype(jnp.float32).reshape(seq_total, HEADS, VDIM))
    g_query = d_query.reshape(seq_total, HEADS * KDIM).astype(jnp.bfloat16)
    g_fwd = d_fwd.reshape(seq_total, HEADS * KDIM).astype(jnp.bfloat16)
    g_bwd = d_bwd.reshape(seq_total, HEADS * KDIM).astype(jnp.bfloat16)
    g_value = d_value.reshape(seq_total, HEADS * VDIM).astype(jnp.bfloat16)
    summed = jnp.dot(g_query, w_query.T, preferred_element_type=jnp.float32)
    summed = summed + jnp.dot(g_fwd, w_forget_fwd.T, preferred_element_type=jnp.float32)
    summed = summed + jnp.dot(g_bwd, w_forget_bwd.T, preferred_element_type=jnp.float32)
    summed = summed + jnp.dot(g_value, w_value.T, preferred_element_type=jnp.float32)
    norm_scale = seq_total ** (-0.5)
    grad_weight = jnp.dot(block_input.T, g_query, preferred_element_type=jnp.float32) * norm_scale
    grad_floor = d_rates.reshape(2, HEADS * KDIM) * norm_scale
    return (summed.astype(jnp.bfloat16), grad_weight, grad_floor)
```

```python
import functools

import jax
import jax.numpy as jnp
from jax import lax
from jax.experimental import pallas as pl
from jax.experimental.pallas import tpu as pltpu
from jax.sharding import PartitionSpec as P

KDIM = 128
NORM_EPS = 1e-06
MESH = pl.DeviceIdType.MESH
F32 = jnp.float32
BF16 = jnp.bfloat16

NN = (((1,), (0,)), ((), ()))
NT = (((1,), (1,)), ((), ()))
TN = (((0,), (0,)), ((), ()))


def dot(a, b, dims):
    return lax.dot_general(a, b, dims, preferred_element_type=F32)


def split(a):
    high = a.astype(BF16)
    return high, (a - high.astype(F32)).astype(BF16)


def mm(a, b, dims):
    if not isinstance(a, tuple):
        return dot(a, b[0], dims) + dot(a, b[1], dims)
    if not isinstance(b, tuple):
        return dot(a[0], b, dims) + dot(a[1], b, dims)
    return dot(a[0], b[0], dims) + (dot(a[1], b[0], dims) + dot(a[0], b[1], dims))


def gates(raw, rate):
    opening = rate * (1.0 - rate * (0.5 - rate * (1.0 / 6.0 - rate * (1.0 / 24.0 - rate * (1.0 / 120.0)))))
    small = jnp.exp(-jnp.abs(raw))
    inverse = 1.0 / (1.0 + small)
    other = small * inverse
    positive = raw >= 0
    sig_pos = jnp.where(positive, inverse, other)
    sig_neg = jnp.where(positive, other, inverse)
    key = opening * sig_neg
    log_forget = -key * (1.0 + key * (0.5 + key * (1.0 / 3.0 + key * (0.25 + key * 0.2))))
    return key, log_forget, sig_pos, sig_neg, opening


def kernel(
    n_sp, n_tp, heads, seq_total,
    x_hbm, wq_hbm, wf_hbm, wb_hbm, wv_hbm, ct_hbm, rate_ref, gain_ref,
    gin_ref, gw_ref, gfl_ref,
    x_v, wq_v, wf_v, wb_v, wv_v, ct_v,
    dec_s, dec_r, a1_s, a1_r, a2_s, a2_r, b1_s, b1_r, b2_s, b2_r,
    w1_s, w1_r, w2_s, w2_r, y_s, rel_r, ysum_s, y_r, fl_s, fl_r,
    in_sem, snd, rcv, y_snd, y_rcv,
):
    me = lax.axis_index("sp")
    tp = lax.axis_index("tp")
    core = lax.rem(me, 2)
    chip = lax.div(me, 2)
    n_chip = n_sp // 2
    tok = x_hbm.shape[0]
    width = x_hbm.shape[1]
    per = n_sp // heads
    my_head = lax.div(me, per)
    q_scale = KDIM ** (-0.5)
    norm_scale = seq_total ** (-0.5)

    loads = [
        pltpu.make_async_copy(src, dst, in_sem.at[i])
        for i, (src, dst) in enumerate(
            [(x_hbm, x_v), (wf_hbm, wf_v), (wb_hbm, wb_v), (wv_hbm, wv_v), (wq_hbm, wq_v), (ct_hbm, ct_v)]
        )
    ]
    for load in loads:
        load.start()

    right = (me, lax.rem(tp + 1, n_tp))
    left = (me, lax.rem(tp + n_tp - 1, n_tp))
    barrier = pltpu.get_barrier_semaphore()

    def greet(r, c):
        pl.semaphore_signal(barrier, inc=1, device_id=(lax.rem(me + r, n_sp), tp), device_id_type=MESH)
        return c

    lax.fori_loop(1, n_sp, greet, 0)
    pl.semaphore_signal(barrier, inc=1, device_id=right, device_id_type=MESH)
    pl.semaphore_signal(barrier, inc=1, device_id=left, device_id_type=MESH)

    def spread(source_of, landing, i, count=n_sp, device_of=None):
        mine = me if count == n_sp else chip

        def step(r, c):
            to = lax.rem(mine + r, count)
            device = (to, tp) if count == n_sp else (to * 2 + core, tp)
            pltpu.make_async_remote_copy(
                src_ref=source_of(to), dst_ref=landing.at[count - r],
                send_sem=snd.at[i], recv_sem=rcv.at[i], device_id=device, device_id_type=MESH,
            ).start()
            return c

        lax.fori_loop(1, count, step, 0)

    def whole(landing, i, count=n_sp):
        part = landing.at[pl.ds(1, count - 1)]
        return pltpu.make_async_remote_copy(
            src_ref=part, dst_ref=part, send_sem=snd.at[i], recv_sem=rcv.at[i],
            device_id=(me, tp), device_id_type=MESH,
        )

    def place(j):
        return lax.rem(j - me + n_sp, n_sp)

    row = lax.broadcasted_iota(jnp.int32, (tok, tok), 0)
    col = lax.broadcasted_iota(jnp.int32, (tok, tok), 1)
    lower = col <= row
    upper = col >= row
    lower_ones = jnp.where(lower, 1.0, 0.0).astype(BF16)
    upper_ones = jnp.where(upper, 1.0, 0.0).astype(BF16)

    loads[0].wait()
    loads[1].wait()
    x = x_v[...]
    raw_f = dot(x, wf_v[...], NN).astype(BF16).astype(F32)
    loads[2].wait()
    raw_b = dot(x, wb_v[...], NN).astype(BF16).astype(F32)
    rate = rate_ref[...] * (1.0 / seq_total)
    key_f, log_f, sp_f, sn_f, open_f = gates(raw_f, rate[0:1])
    key_b, log_b, sp_b, sn_b, open_b = gates(raw_b, rate[1:2])
    cum_f = mm(lower_ones, split(log_f), NN)
    cum_b = mm(upper_ones, split(log_b), NN)
    dec_f = jnp.exp(cum_f[tok - 1 : tok])
    dec_b = jnp.exp(cum_b[0:1])
    head = lambda a, h: a[:, h * KDIM : (h + 1) * KDIM]
    for h in range(heads):
        dec_s[h, 0:1, :] = head(dec_f, h)
        dec_s[h, 1:2, :] = head(dec_b, h)
    pl.semaphore_wait(barrier, n_sp + 1)
    spread(lambda to: dec_s.at[lax.div(to, per)], dec_r, 0)
    dec_r[0] = dec_s[my_head]

    grow_f, grow_b = jnp.exp(-cum_f), jnp.exp(-cum_b)
    kd_f, kd_b = key_f * grow_f, key_b * grow_b
    kx_f, kx_b = kd_f * dec_f, kd_b * dec_b
    loads[3].wait()
    v = dot(x, wv_v[...], NN).astype(BF16)
    for h in range(heads):
        kx = split(jnp.concatenate([head(kx_f, h), head(kx_b, h)], axis=1))
        local = mm(head(v, h), kx, TN)
        a1_s[pl.ds(h * per, per), 0:8, :] = local[:, :KDIM].reshape(per, 8, KDIM)
        a1_s[pl.ds(h * per, per), 8:16, :] = local[:, KDIM:].reshape(per, 8, KDIM)

    spread(lambda to: a1_s.at[to], a1_r, 1)
    a1_r[0] = a1_s[me]

    loads[4].wait()
    q = dot(x, wq_v[...], NN).astype(BF16).astype(F32) * q_scale
    fade_f, fade_b = jnp.exp(cum_f), jnp.exp(cum_b)
    q_f, q_b = q * fade_f, q * fade_b
    q_fs = [split(head(q_f, h)) for h in range(heads)]
    q_bs = [split(head(q_b, h)) for h in range(heads)]
    kd_fs = [split(head(kd_f, h)) for h in range(heads)]
    kd_bs = [split(head(kd_b, h)) for h in range(heads)]
    scores = []
    inner = []
    for h in range(heads):
        score = jnp.where(lower, mm(q_fs[h], kd_fs[h], NT), 0.0) + jnp.where(upper, mm(q_bs[h], kd_bs[h], NT), 0.0)
        scores.append(split(score))
        inner.append(mm(scores[h], head(v, h), NN))

    def owner_scan(received, result, up_rows, up_dir, down_rows, down_dir):
        up = jnp.zeros((8, KDIM), F32)
        down = jnp.zeros((8, KDIM), F32)
        for i in range(n_sp):
            j, jj = i, n_sp - 1 - i
            slot, back = place(j), place(jj)
            result[j, up_rows, :] = up
            result[jj, down_rows, :] = down
            if i < n_sp - 1:
                up = up * dec_r[slot, up_dir : up_dir + 1, :] + received[slot, up_rows, :]
                down = down * dec_r[back, down_dir : down_dir + 1, :] + received[back, down_rows, :]

    FWD, BWD = slice(0, 8), slice(8, 16)

    def give_back(result, landing, i):
        def step(r, c):
            to = lax.rem(me + r, n_sp)
            pltpu.make_async_remote_copy(
                src_ref=result.at[to], dst_ref=landing.at[me],
                send_sem=snd.at[i], recv_sem=rcv.at[i], device_id=(to, tp), device_id_type=MESH,
            ).start()
            return c

        lax.fori_loop(1, n_sp, step, 0)
        landing[me] = result[me]

    whole(dec_r, 0).wait_recv()
    whole(a1_r, 1).wait_recv()
    owner_scan(a1_r, a2_s, FWD, 0, BWD, 1)
    give_back(a2_s, a2_r, 2)
    loads[5].wait()
    cot = ct_v[...].astype(F32)
    gain = gain_ref[...]
    whole(a2_r, 2).wait_recv()

    def state(buf, h, rows):
        return buf[pl.ds(h * per, per), rows, :].reshape(KDIM, KDIM)

    both = [split(jnp.concatenate([state(a2_r, h, FWD), state(a2_r, h, BWD)], axis=1)) for h in range(heads)]
    q_both = [tuple(jnp.concatenate([q_fs[h][i], q_bs[h][i]], axis=1) for i in range(2)) for h in range(heads)]
    d_out = []
    for h in range(heads):
        mixed = inner[h] + mm(q_both[h], both[h], NT)
        inv = lax.rsqrt(jnp.mean(mixed * mixed, axis=-1, keepdims=True) + NORM_EPS)
        scaled = head(cot, h) * gain
        pull = jnp.mean(mixed * scaled, axis=-1, keepdims=True)
        d_mixed = inv * scaled - mixed * (inv * inv * inv * pull)
        d_out.append(split(d_mixed))
        seed = mm(d_out[h], q_both[h], TN)
        b1_s[pl.ds(h * per, per), 0:8, :] = seed[:, :KDIM].reshape(per, 8, KDIM)
        b1_s[pl.ds(h * per, per), 8:16, :] = seed[:, KDIM:].reshape(per, 8, KDIM)
    spread(lambda to: b1_s.at[to], b1_r, 3)
    b1_r[0] = b1_s[me]

    dq_f, dq_b, d_low, d_high = [], [], [], []
    for h in range(heads):
        d_score = mm(d_out[h], head(v, h), NT)
        low = split(jnp.where(lower, d_score, 0.0))
        high = split(jnp.where(upper, d_score, 0.0))
        outer = mm(d_out[h], both[h], NN)
        dq_f.append(mm(low, kd_fs[h], NN) + outer[:, :KDIM])
        dq_b.append(mm(high, kd_bs[h], NN) + outer[:, KDIM:])
        d_low.append(low)
        d_high.append(high)
    cat = lambda parts: jnp.concatenate(parts, axis=1)
    dq_f, dq_b = cat(dq_f), cat(dq_b)
    g_q = ((dq_f * fade_f + dq_b * fade_b) * q_scale).astype(BF16)
    rows_w = width // n_sp
    for i in range(width // KDIM):
        block = dot(x_v[:, i * KDIM : (i + 1) * KDIM], g_q, TN)
        for k in range(KDIM // rows_w):
            p = i * (KDIM // rows_w) + k
            w1_s[p % 2, p // 2] = block[k * rows_w : (k + 1) * rows_w]
    sibling = pltpu.make_async_remote_copy(
        src_ref=w1_s.at[1 - core], dst_ref=w1_r, send_sem=snd.at[5], recv_sem=rcv.at[5],
        device_id=(me + 1 - 2 * core, tp), device_id_type=MESH,
    )
    sibling.start()
    dk_f = cat([mm(d_low[h], q_fs[h], TN) for h in range(heads)])
    dk_b = cat([mm(d_high[h], q_bs[h], TN) for h in range(heads)])
    dv = [mm(scores[h], d_out[h], TN) for h in range(heads)]

    whole(b1_r, 3).wait_recv()
    owner_scan(b1_r, b2_s, BWD, 1, FWD, 0)
    give_back(b2_s, b2_r, 4)

    sibling.wait_recv()
    w2_s[...] = w1_s[core] + w1_r[...]
    spread(lambda to: w2_s.at[to], w2_r, 6, n_chip)

    whole(b2_r, 4).wait_recv()
    dx_f, dx_b, edge_f, edge_b = [], [], [], []
    for h in range(heads):
        back_f, back_b = state(b2_r, h, FWD), state(b2_r, h, BWD)
        back = split(jnp.concatenate([back_f, back_b], axis=1))
        dx = mm(head(v, h), back, NN)
        dx_f.append(dx[:, :KDIM])
        dx_b.append(dx[:, KDIM:])
        kx = split(jnp.concatenate([head(kx_f, h), head(kx_b, h)], axis=1))
        dv[h] = dv[h] + mm(kx, back, NT)
        leave_f = head(dec_f, h) * state(a2_r, h, FWD) + state(a1_s, h, FWD)
        leave_b = head(dec_b, h) * state(a2_r, h, BWD) + state(a1_s, h, BWD)
        edge_f.append(jnp.sum(leave_f * back_f, axis=0, keepdims=True))
        edge_b.append(jnp.sum(leave_b * back_b, axis=0, keepdims=True))
    dx_f, dx_b, edge_f, edge_b = cat(dx_f), cat(dx_b), cat(edge_f), cat(edge_b)

    def gate_back(dk, dx, dq, kd, kx, q_d, grow, dec, edge, ones, key, sig_pos, sig_neg, opening):
        along = q_d * dq - kd * dk - kx * dx
        d_log = mm(ones, split(along), NN) + edge
        d_key = grow * (dk + dec * dx) - d_log / (1.0 - key)
        d_raw = -d_key * key * sig_pos
        d_rate = jnp.sum(d_key * sig_neg, axis=0, keepdims=True) * ((1.0 - opening) * (1.0 / seq_total))
        return d_raw.astype(BF16), d_rate

    g_f, r_f = gate_back(dk_f, dx_f, dq_f, kd_f, kx_f, q_f, grow_f, dec_f, edge_f, upper_ones, key_f, sp_f, sn_f, open_f)
    g_b, r_b = gate_back(dk_b, dx_b, dq_b, kd_b, kx_b, q_b, grow_b, dec_b, edge_b, lower_ones, key_b, sp_b, sn_b, open_b)
    g_v = cat(dv).astype(BF16)
    for h in range(heads):
        fl_s[h : h + 1, :] = head(r_f, h)
        fl_s[heads + h : heads + h + 1, :] = head(r_b, h)
    spread(lambda to: fl_s, fl_r, 7)
    fl_r[0] = fl_s[...]

    rows_y = tok // n_tp
    half = width // 2
    for part in range(2):
        cols = pl.ds(part * half, half)
        y = (
            dot(g_q, wq_v[cols, :], NT)
            + dot(g_f, wf_v[cols, :], NT)
            + dot(g_b, wb_v[cols, :], NT)
            + dot(g_v, wv_v[cols, :], NT)
        )
        y_s[part] = y.reshape(n_tp, rows_y, half)

    up, down, across = lax.rem(tp + 1, n_tp), lax.rem(tp + n_tp - 1, n_tp), lax.rem(tp + 2, n_tp)

    def ring(src, dst, i, device):
        return pltpu.make_async_remote_copy(
            src_ref=src, dst_ref=dst, send_sem=y_snd.at[i], recv_sem=y_rcv.at[i],
            device_id=device, device_id_type=MESH,
        )

    hops = [
        ring(y_s.at[0, across], rel_r.at[0], 0, right),
        ring(y_s.at[1, across], rel_r.at[1], 1, left),
        ring(y_s.at[1, up], y_r.at[0], 2, right),
        ring(y_s.at[0, down], y_r.at[1], 3, left),
        ring(ysum_s.at[0], y_r.at[2], 4, right),
        ring(ysum_s.at[1], y_r.at[3], 5, left),
    ]
    for hop in hops[:4]:
        hop.start()
    hops[0].wait_recv()
    ysum_s[0] = y_s[0, up] + rel_r[0]
    hops[4].start()
    hops[1].wait_recv()
    ysum_s[1] = y_s[1, down] + rel_r[1]
    hops[5].start()

    whole(fl_r, 7).wait_recv()
    total = jnp.zeros((2 * heads, KDIM), F32)
    for j in range(n_sp):
        total = total + fl_r[place(j)]
    total = total * norm_scale
    for h in range(heads):
        gfl_ref[0:1, h * KDIM : (h + 1) * KDIM] = total[h : h + 1]
        gfl_ref[1:2, h * KDIM : (h + 1) * KDIM] = total[heads + h : heads + h + 1]

    whole(w2_r, 6, n_chip).wait_recv()
    acc = w2_s[chip]
    for r in range(1, n_chip):
        acc = acc + w2_r[r]
    gw_ref[...] = acc * norm_scale

    for hop in hops[2:]:
        hop.wait_recv()
    gin_ref[:, 0:half] = (y_s[0, tp] + y_r[2] + y_r[1]).astype(BF16)
    gin_ref[:, half:] = (y_s[1, tp] + y_r[0] + y_r[3]).astype(BF16)

    for landing, i in ((dec_r, 0), (a1_r, 1), (a2_r, 2), (b1_r, 3), (b2_r, 4), (fl_r, 7)):
        whole(landing, i).wait_send()
    whole(w2_r, 6, n_chip).wait_send()
    sibling.wait_send()
    for hop in hops:
        hop.wait_send()


def solution(mesh):
    n_sp, n_tp = mesh.shape["sp"], mesh.shape["tp"]

    def body(block_input, w_query, w_forget_fwd, w_forget_bwd, w_value, floor_rate, gain, cotangent):
        tok, width = block_input.shape
        cols = w_query.shape[1]
        heads = cols // KDIM
        n_chip = n_sp // 2
        rows_w = width // n_sp
        rows_y = tok // n_tp
        half = width // 2
        vm = pltpu.VMEM
        pieces = [vm((n_sp, 16, KDIM), F32) for _ in range(8)]
        any_spec = pl.BlockSpec(memory_space=pl.ANY)
        vmem_spec = pl.BlockSpec(memory_space=pltpu.VMEM)
        return pl.pallas_call(
            functools.partial(kernel, n_sp, n_tp, heads, float(tok * n_sp)),
            out_shape=(
                jax.ShapeDtypeStruct((rows_y, width), BF16),
                jax.ShapeDtypeStruct((rows_w, cols), F32),
                jax.ShapeDtypeStruct((2, cols), F32),
            ),
            in_specs=[any_spec] * 6 + [vmem_spec] * 2,
            out_specs=(vmem_spec,) * 3,
            scratch_shapes=[
                vm((tok, width), BF16),
                vm((width, cols), BF16), vm((width, cols), BF16), vm((width, cols), BF16), vm((width, cols), BF16),
                vm((tok, cols), BF16),
                vm((heads, 2, KDIM), F32), vm((n_sp, 2, KDIM), F32),
                *pieces,
                vm((2, n_chip, rows_w, cols), F32), vm((n_chip, rows_w, cols), F32),
                vm((n_chip, rows_w, cols), F32), vm((n_chip, rows_w, cols), F32),
                vm((2, n_tp, rows_y, half), F32), vm((2, rows_y, half), F32),
                vm((2, rows_y, half), F32), vm((4, rows_y, half), F32),
                vm((2 * heads, KDIM), F32), vm((n_sp, 2 * heads, KDIM), F32),
                pltpu.SemaphoreType.DMA((6,)),
                pltpu.SemaphoreType.DMA((8,)),
                pltpu.SemaphoreType.DMA((8,)),
                pltpu.SemaphoreType.DMA((6,)),
                pltpu.SemaphoreType.DMA((6,)),
            ],
            compiler_params=pltpu.CompilerParams(collective_id=0, has_side_effects=True),
        )(block_input, w_query, w_forget_fwd, w_forget_bwd, w_value, cotangent, floor_rate, gain.reshape(1, KDIM))

    return jax.shard_map(
        body,
        mesh=mesh,
        in_specs=(
            P("sp", None), P(None, "tp"), P(None, "tp"), P(None, "tp"), P(None, "tp"), P(None, "tp"), P(), P("sp", "tp"),
        ),
        out_specs=(P(("sp", "tp"), None), P("sp", "tp"), P(None, "tp")),
        check_vma=False,
    )
```

```python
import functools

import jax
import jax.numpy as jnp
from jax import lax
from jax.experimental import pallas as pl
from jax.experimental.pallas import tpu as pltpu
from jax.sharding import PartitionSpec as P

KDIM = 128
NORM_EPS = 1e-06
MESH = pl.DeviceIdType.MESH
F32 = jnp.float32
BF16 = jnp.bfloat16

NN = (((1,), (0,)), ((), ()))
NT = (((1,), (1,)), ((), ()))
TN = (((0,), (0,)), ((), ()))


def dot(a, b, dims):
    return lax.dot_general(a, b, dims, preferred_element_type=F32)


def split(a):
    high = a.astype(BF16)
    return high, (a - high.astype(F32)).astype(BF16)


def mm(a, b, dims):
    if not isinstance(a, tuple):
        return dot(a, b[0], dims) + dot(a, b[1], dims)
    if not isinstance(b, tuple):
        return dot(a[0], b, dims) + dot(a[1], b, dims)
    return dot(a[0], b[0], dims) + (dot(a[1], b[0], dims) + dot(a[0], b[1], dims))


def gates(raw, rate):
    opening = rate * (1.0 - rate * (0.5 - rate * (1.0 / 6.0 - rate * (1.0 / 24.0 - rate * (1.0 / 120.0)))))
    small = jnp.exp(-jnp.abs(raw))
    inverse = 1.0 / (1.0 + small)
    other = small * inverse
    positive = raw >= 0
    sig_pos = jnp.where(positive, inverse, other)
    sig_neg = jnp.where(positive, other, inverse)
    key = opening * sig_neg
    log_forget = -key * (1.0 + key * (0.5 + key * (1.0 / 3.0 + key * (0.25 + key * 0.2))))
    return key, log_forget, sig_pos, sig_neg, opening


def kernel(
    n_sp, n_tp, heads, seq_total,
    x_hbm, wq_hbm, wf_hbm, wb_hbm, wv_hbm, ct_hbm, rate_ref, gain_ref,
    gin_ref, gw_ref, gfl_ref,
    x_v, wq_v, wf_v, wb_v, wv_v, ct_v,
    dec_s, dec_r, a1_s, a1_r, a2_s, a2_r, b1_s, b1_r, b2_s, b2_r,
    w1_s, w1_r, w2_s, w2_r, y_s, rel_r, ysum_s, y_r, fl_s, fl_r,
    in_sem, snd, rcv, y_snd, y_rcv,
):
    me = lax.axis_index("sp")
    tp = lax.axis_index("tp")
    core = lax.rem(me, 2)
    chip = lax.div(me, 2)
    n_chip = n_sp // 2
    tok = x_hbm.shape[0]
    width = x_hbm.shape[1]
    per = n_sp // heads
    my_head = lax.div(me, per)
    q_scale = KDIM ** (-0.5)
    norm_scale = seq_total ** (-0.5)

    loads = [
        pltpu.make_async_copy(src, dst, in_sem.at[i])
        for i, (src, dst) in enumerate(
            [(x_hbm, x_v), (wf_hbm, wf_v), (wb_hbm, wb_v), (wv_hbm, wv_v), (wq_hbm, wq_v), (ct_hbm, ct_v)]
        )
    ]
    for load in loads:
        load.start()
    loading = dict(enumerate(loads))
    flying, sent = {}, []

    def loaded(i):
        loading.pop(i).wait()

    def begun(name, copy):
        flying[name] = copy
        sent.append(copy)

    def arrived(name):
        flying.pop(name).wait_recv()

    def drain():
        for name in list(flying):
            arrived(name)
        for i in list(loading):
            loaded(i)
        for copy in sent:
            copy.wait_send()

    right = (me, lax.rem(tp + 1, n_tp))
    left = (me, lax.rem(tp + n_tp - 1, n_tp))
    barrier = pltpu.get_barrier_semaphore()

    def greet(r, c):
        pl.semaphore_signal(barrier, inc=1, device_id=(lax.rem(me + r, n_sp), tp), device_id_type=MESH)
        return c

    lax.fori_loop(1, n_sp, greet, 0)
    pl.semaphore_signal(barrier, inc=1, device_id=right, device_id_type=MESH)
    pl.semaphore_signal(barrier, inc=1, device_id=left, device_id_type=MESH)

    def put(src, dst, i, device):
        pltpu.make_async_remote_copy(
            src_ref=src, dst_ref=dst, send_sem=snd.at[i], recv_sem=rcv.at[i],
            device_id=device, device_id_type=MESH,
        ).start()

    def took(part, i):
        return pltpu.make_async_remote_copy(
            src_ref=part, dst_ref=part, send_sem=snd.at[i], recv_sem=rcv.at[i],
            device_id=(me, tp), device_id_type=MESH,
        )

    def to_all(source_of, landing, i):
        def step(r, c):
            to = lax.rem(me + r, n_sp)
            put(source_of(to), landing.at[me], i, (to, tp))
            return c

        lax.fori_loop(1, n_sp, step, 0)
        begun(i, took(landing.at[pl.ds(0, n_sp - 1)], i))

    def to_owners(source, landing, i, h):
        mine = lax.rem(me, per)

        def step(r, c):
            to = h * per + lax.rem(mine + r, per)
            put(source.at[to], landing.at[me], i, (to, tp))
            return c

        lax.fori_loop(jnp.where(my_head == h, 1, 0), per, step, 0)
        if h == heads - 1:
            begun(i, took(landing.at[pl.ds(0, n_sp - 1)], i))
            landing[me] = source[me]

    def give_back(result, landing, i):
        def step(r, c):
            to = lax.rem(me + r, n_sp)
            pltpu.make_async_remote_copy(
                src_ref=result.at[to], dst_ref=landing.at[me], send_sem=snd.at[i], recv_sem=rcv.at[i + my_head],
                device_id=(to, tp), device_id_type=MESH,
            ).start()
            return c

        lax.fori_loop(1, n_sp, step, 0)
        sent.append(took(landing.at[pl.ds(0, n_sp - 1)], i))
        landing[me] = result[me]

    def head_arrived(landing, i, h):
        @pl.when(my_head == h)
        def _():
            took(landing.at[pl.ds(h * per, per - 1)], i + h).wait_recv()

        @pl.when(my_head != h)
        def _():
            took(landing.at[pl.ds(h * per, per)], i + h).wait_recv()

    row = lax.broadcasted_iota(jnp.int32, (tok, tok), 0)
    col = lax.broadcasted_iota(jnp.int32, (tok, tok), 1)
    lower = col <= row
    upper = col >= row
    lower_ones = jnp.where(lower, 1.0, 0.0).astype(BF16)
    upper_ones = jnp.where(upper, 1.0, 0.0).astype(BF16)

    loaded(0)
    loaded(1)
    x = x_v[...]
    raw_f = dot(x, wf_v[...], NN).astype(BF16).astype(F32)
    loaded(2)
    raw_b = dot(x, wb_v[...], NN).astype(BF16).astype(F32)
    rate = rate_ref[...] * (1.0 / seq_total)
    key_f, log_f, sp_f, sn_f, open_f = gates(raw_f, rate[0:1])
    key_b, log_b, sp_b, sn_b, open_b = gates(raw_b, rate[1:2])
    cum_f = mm(lower_ones, split(log_f), NN)
    cum_b = mm(upper_ones, split(log_b), NN)
    dec_f = jnp.exp(cum_f[tok - 1 : tok])
    dec_b = jnp.exp(cum_b[0:1])
    head = lambda a, h: a[:, h * KDIM : (h + 1) * KDIM]
    for h in range(heads):
        dec_s[h, 0:1, :] = head(dec_f, h)
        dec_s[h, 1:2, :] = head(dec_b, h)
    dec_r[me] = dec_s[my_head]

    grow_f, grow_b = jnp.exp(-cum_f), jnp.exp(-cum_b)
    kd_f, kd_b = key_f * grow_f, key_b * grow_b
    kx_f, kx_b = kd_f * dec_f, kd_b * dec_b
    loaded(3)
    v = dot(x, wv_v[...], NN).astype(BF16)
    for h in range(heads):
        kx = split(jnp.concatenate([head(kx_f, h), head(kx_b, h)], axis=1))
        local = mm(head(v, h), kx, TN)
        a1_s[pl.ds(h * per, per), 0:8, :] = local[:, :KDIM].reshape(per, 8, KDIM)
        a1_s[pl.ds(h * per, per), 8:16, :] = local[:, KDIM:].reshape(per, 8, KDIM)

    pl.semaphore_wait(barrier, n_sp + 1)
    for h in range(heads):
        to_owners(a1_s, a1_r, 1, h)
    to_all(lambda to: dec_s.at[lax.div(to, per)], dec_r, 0)

    loaded(4)
    q = dot(x, wq_v[...], NN).astype(BF16).astype(F32) * q_scale
    fade_f, fade_b = jnp.exp(cum_f), jnp.exp(cum_b)
    q_f, q_b = q * fade_f, q * fade_b
    q_fs = [split(head(q_f, h)) for h in range(heads)]
    q_bs = [split(head(q_b, h)) for h in range(heads)]
    kd_fs = [split(head(kd_f, h)) for h in range(heads)]
    kd_bs = [split(head(kd_b, h)) for h in range(heads)]
    scores = []
    inner = []
    for h in range(heads):
        score = jnp.where(lower, mm(q_fs[h], kd_fs[h], NT), 0.0) + jnp.where(upper, mm(q_bs[h], kd_bs[h], NT), 0.0)
        scores.append(split(score))
        inner.append(mm(scores[h], head(v, h), NN))

    def owner_scan(received, result, up_rows, up_dir, down_rows, down_dir):
        up = jnp.zeros((8, KDIM), F32)
        down = jnp.zeros((8, KDIM), F32)
        for j in range(n_sp):
            k = n_sp - 1 - j
            result[j, up_rows, :] = up
            result[k, down_rows, :] = down
            if j < n_sp - 1:
                up = up * dec_r[j, up_dir : up_dir + 1, :] + received[j, up_rows, :]
                down = down * dec_r[k, down_dir : down_dir + 1, :] + received[k, down_rows, :]

    FWD, BWD = slice(0, 8), slice(8, 16)

    arrived(0)
    arrived(1)
    owner_scan(a1_r, a2_s, FWD, 0, BWD, 1)
    give_back(a2_s, a2_r, 2)
    loaded(5)
    cot = ct_v[...].astype(F32)
    gain = gain_ref[...]
    def state(buf, h, rows):
        return buf[pl.ds(h * per, per), rows, :].reshape(KDIM, KDIM)

    q_both = [tuple(jnp.concatenate([q_fs[h][i], q_bs[h][i]], axis=1) for i in range(2)) for h in range(heads)]
    both, d_out = [], []
    for h in range(heads):
        head_arrived(a2_r, 2, h)
        both.append(split(jnp.concatenate([state(a2_r, h, FWD), state(a2_r, h, BWD)], axis=1)))
        mixed = inner[h] + mm(q_both[h], both[h], NT)
        inv = lax.rsqrt(jnp.mean(mixed * mixed, axis=-1, keepdims=True) + NORM_EPS)
        scaled = head(cot, h) * gain
        pull = jnp.mean(mixed * scaled, axis=-1, keepdims=True)
        d_mixed = inv * scaled - mixed * (inv * inv * inv * pull)
        d_out.append(split(d_mixed))
        seed = mm(d_out[h], q_both[h], TN)
        b1_s[pl.ds(h * per, per), 0:8, :] = seed[:, :KDIM].reshape(per, 8, KDIM)
        b1_s[pl.ds(h * per, per), 8:16, :] = seed[:, KDIM:].reshape(per, 8, KDIM)
        to_owners(b1_s, b1_r, 4, h)

    dq_f, dq_b, d_low, d_high = [], [], [], []
    for h in range(heads):
        d_score = mm(d_out[h], head(v, h), NT)
        low = split(jnp.where(lower, d_score, 0.0))
        high = split(jnp.where(upper, d_score, 0.0))
        outer = mm(d_out[h], both[h], NN)
        dq_f.append(mm(low, kd_fs[h], NN) + outer[:, :KDIM])
        dq_b.append(mm(high, kd_bs[h], NN) + outer[:, KDIM:])
        d_low.append(low)
        d_high.append(high)
    cat = lambda parts: jnp.concatenate(parts, axis=1)
    g_q = ((cat(dq_f) * fade_f + cat(dq_b) * fade_b) * q_scale).astype(BF16)
    rows_w = width // n_sp
    for i in range(width // KDIM):
        block = dot(x_v[:, i * KDIM : (i + 1) * KDIM], g_q, TN)
        for k in range(KDIM // rows_w):
            p = i * (KDIM // rows_w) + k
            w1_s[p % 2, p // 2] = block[k * rows_w : (k + 1) * rows_w]
    sibling = pltpu.make_async_remote_copy(
        src_ref=w1_s.at[1 - core], dst_ref=w1_r, send_sem=snd.at[7], recv_sem=rcv.at[7],
        device_id=(me + 1 - 2 * core, tp), device_id_type=MESH,
    )
    sibling.start()
    begun(7, sibling)
    dk_f = [mm(d_low[h], q_fs[h], TN) for h in range(heads)]
    dk_b = [mm(d_high[h], q_bs[h], TN) for h in range(heads)]
    dv = [mm(scores[h], d_out[h], TN) for h in range(heads)]
    quarter = width // 4
    rows_y = tok // n_tp
    for c in range(4):
        y_s[c] = dot(g_q, wq_v[c * quarter : (c + 1) * quarter, :], NT).reshape(n_tp, rows_y, quarter)

    arrived(4)
    owner_scan(b1_r, b2_s, BWD, 1, FWD, 0)
    give_back(b2_s, b2_r, 5)

    arrived(7)
    w2_s[...] = w1_s[core] + w1_r[...]

    def to_chip(r, c):
        to = lax.rem(chip + r, n_chip)
        put(w2_s.at[to], w2_r.at[n_chip - r], 8, (to * 2 + core, tp))
        return c

    lax.fori_loop(1, n_chip, to_chip, 0)
    begun(8, took(w2_r.at[pl.ds(1, n_chip - 1)], 8))

    def gate_back(dk, dx, dq, kd, kx, q_d, grow, dec, edge, ones, key, sig_pos, sig_neg, opening):
        along = q_d * dq - kd * dk - kx * dx
        d_log = mm(ones, split(along), NN) + edge
        d_key = grow * (dk + dec * dx) - d_log / (1.0 - key)
        d_raw = -d_key * key * sig_pos
        d_rate = jnp.sum(d_key * sig_neg, axis=0, keepdims=True) * ((1.0 - opening) * (1.0 / seq_total))
        return d_raw.astype(BF16), d_rate

    for h in range(heads):
        head_arrived(b2_r, 5, h)
        back_f, back_b = state(b2_r, h, FWD), state(b2_r, h, BWD)
        back = split(jnp.concatenate([back_f, back_b], axis=1))
        dx = mm(head(v, h), back, NN)
        kx = split(jnp.concatenate([head(kx_f, h), head(kx_b, h)], axis=1))
        g_v = (dv[h] + mm(kx, back, NT)).astype(BF16)
        leave_f = head(dec_f, h) * state(a2_r, h, FWD) + state(a1_s, h, FWD)
        leave_b = head(dec_b, h) * state(a2_r, h, BWD) + state(a1_s, h, BWD)
        edge_f = jnp.sum(leave_f * back_f, axis=0, keepdims=True)
        edge_b = jnp.sum(leave_b * back_b, axis=0, keepdims=True)
        here = lambda *arrays: [head(a, h) for a in arrays]
        g_f, r_f = gate_back(
            dk_f[h], dx[:, :KDIM], dq_f[h], *here(kd_f, kx_f, q_f, grow_f, dec_f), edge_f,
            upper_ones, *here(key_f, sp_f, sn_f, open_f),
        )
        g_b, r_b = gate_back(
            dk_b[h], dx[:, KDIM:], dq_b[h], *here(kd_b, kx_b, q_b, grow_b, dec_b), edge_b,
            lower_ones, *here(key_b, sp_b, sn_b, open_b),
        )
        fl_s[h : h + 1, :] = r_f
        fl_s[heads + h : heads + h + 1, :] = r_b
        mine = slice(h * KDIM, (h + 1) * KDIM)
        for c in range(4):
            rows = slice(c * quarter, (c + 1) * quarter)
            y = (
                dot(g_f, wf_v[rows, mine], NT)
                + dot(g_b, wb_v[rows, mine], NT)
                + dot(g_v, wv_v[rows, mine], NT)
            )
            y_s[c] = y_s[c] + y.reshape(n_tp, rows_y, quarter)

    up, down, across = lax.rem(tp + 1, n_tp), lax.rem(tp + n_tp - 1, n_tp), lax.rem(tp + 2, n_tp)

    def ring(src, dst, i, device):
        return pltpu.make_async_remote_copy(
            src_ref=src, dst_ref=dst, send_sem=y_snd.at[i], recv_sem=y_rcv.at[i],
            device_id=device, device_id_type=MESH,
        )

    relay, direct, summed = [], [], []
    for c in range(4):
        ahead, behind = (right, left) if c % 2 == 0 else (left, right)
        relay.append(ring(y_s.at[c, across], rel_r.at[c], c, ahead))
        direct.append(ring(y_s.at[c, down if c % 2 == 0 else up], y_r.at[c], 4 + c, behind))
        summed.append(ring(ysum_s.at[c], y_r.at[4 + c], 8 + c, ahead))
    for c in range(4):
        relay[c].start()
        begun(("relay", c), relay[c])
    for c in range(4):
        direct[c].start()
        begun(("direct", c), direct[c])
    to_all(lambda to: fl_s, fl_r, 9)
    fl_r[me] = fl_s[...]
    for c in range(4):
        arrived(("relay", c))
        ysum_s[c] = y_s[c, up if c % 2 == 0 else down] + rel_r[c]
        summed[c].start()
        begun(("summed", c), summed[c])

    arrived(9)
    total = fl_r[0]
    for j in range(1, n_sp):
        total = total + fl_r[j]
    total = total * norm_scale
    for h in range(heads):
        gfl_ref[0:1, h * KDIM : (h + 1) * KDIM] = total[h : h + 1]
        gfl_ref[1:2, h * KDIM : (h + 1) * KDIM] = total[heads + h : heads + h + 1]

    arrived(8)
    acc = w2_s[chip]
    for r in range(1, n_chip):
        acc = acc + w2_r[r]
    gw_ref[...] = acc * norm_scale

    for c in range(4):
        arrived(("direct", c))
        arrived(("summed", c))
        gin_ref[:, c * quarter : (c + 1) * quarter] = (y_s[c, tp] + y_r[c] + y_r[4 + c]).astype(BF16)

    drain()


def solution(mesh):
    n_sp, n_tp = mesh.shape["sp"], mesh.shape["tp"]

    def body(block_input, w_query, w_forget_fwd, w_forget_bwd, w_value, floor_rate, gain, cotangent):
        tok, width = block_input.shape
        cols = w_query.shape[1]
        heads = cols // KDIM
        n_chip = n_sp // 2
        rows_w = width // n_sp
        rows_y = tok // n_tp
        quarter = width // 4
        vm = pltpu.VMEM
        pieces = [vm((n_sp, 16, KDIM), F32) for _ in range(8)]
        any_spec = pl.BlockSpec(memory_space=pl.ANY)
        vmem_spec = pl.BlockSpec(memory_space=pltpu.VMEM)
        return pl.pallas_call(
            functools.partial(kernel, n_sp, n_tp, heads, float(tok * n_sp)),
            out_shape=(
                pltpu.VMEM((rows_y, width), BF16),
                pltpu.VMEM((rows_w, cols), F32),
                pltpu.VMEM((2, cols), F32),
            ),
            in_specs=[any_spec] * 6 + [vmem_spec] * 2,
            out_specs=(vmem_spec,) * 3,
            scratch_shapes=[
                vm((tok, width), BF16),
                vm((width, cols), BF16), vm((width, cols), BF16), vm((width, cols), BF16), vm((width, cols), BF16),
                vm((tok, cols), BF16),
                vm((heads, 2, KDIM), F32), vm((n_sp, 2, KDIM), F32),
                *pieces,
                vm((2, n_chip, rows_w, cols), F32), vm((n_chip, rows_w, cols), F32),
                vm((n_chip, rows_w, cols), F32), vm((n_chip, rows_w, cols), F32),
                vm((4, n_tp, rows_y, quarter), F32), vm((4, rows_y, quarter), F32),
                vm((4, rows_y, quarter), F32), vm((8, rows_y, quarter), F32),
                vm((2 * heads, KDIM), F32), vm((n_sp, 2 * heads, KDIM), F32),
                pltpu.SemaphoreType.DMA((6,)),
                pltpu.SemaphoreType.DMA((10,)),
                pltpu.SemaphoreType.DMA((10,)),
                pltpu.SemaphoreType.DMA((12,)),
                pltpu.SemaphoreType.DMA((12,)),
            ],
            compiler_params=pltpu.CompilerParams(collective_id=0, has_side_effects=True),
        )(block_input, w_query, w_forget_fwd, w_forget_bwd, w_value, cotangent, floor_rate, gain.reshape(1, KDIM))

    return jax.shard_map(
        body,
        mesh=mesh,
        in_specs=(
            P("sp", None), P(None, "tp"), P(None, "tp"), P(None, "tp"), P(None, "tp"), P(None, "tp"), P(), P("sp", "tp"),
        ),
        out_specs=(P(("sp", "tp"), None), P("sp", "tp"), P(None, "tp")),
        check_vma=False,
    )
```

```python
import functools

import jax
import jax.numpy as jnp
from jax import lax
from jax.experimental import pallas as pl
from jax.experimental.pallas import tpu as pltpu
from jax.sharding import PartitionSpec as P

KDIM = 128
NORM_EPS = 1e-06
MESH = pl.DeviceIdType.MESH
F32 = jnp.float32
BF16 = jnp.bfloat16

NN = (((1,), (0,)), ((), ()))
NT = (((1,), (1,)), ((), ()))
TN = (((0,), (0,)), ((), ()))


def dot(a, b, dims):
    return lax.dot_general(a, b, dims, preferred_element_type=F32)


def split(a):
    high = a.astype(BF16)
    return high, (a - high.astype(F32)).astype(BF16)


def mm(a, b, dims):
    if not isinstance(a, tuple):
        return dot(a, b[0], dims) + dot(a, b[1], dims)
    if not isinstance(b, tuple):
        return dot(a[0], b, dims) + dot(a[1], b, dims)
    return dot(a[0], b[0], dims) + (dot(a[1], b[0], dims) + dot(a[0], b[1], dims))


def gates(raw, rate):
    opening = rate * (1.0 - rate * (0.5 - rate * (1.0 / 6.0 - rate * (1.0 / 24.0 - rate * (1.0 / 120.0)))))
    small = jnp.exp(-jnp.abs(raw))
    inverse = 1.0 / (1.0 + small)
    other = small * inverse
    positive = raw >= 0
    sig_pos = jnp.where(positive, inverse, other)
    sig_neg = jnp.where(positive, other, inverse)
    key = opening * sig_neg
    log_forget = -key * (1.0 + key * (0.5 + key * (1.0 / 3.0 + key * (0.25 + key * 0.2))))
    return key, log_forget, sig_pos, sig_neg, opening


def kernel(
    n_sp, n_tp, heads, seq_total,
    x_hbm, wq_hbm, wf_hbm, wb_hbm, wv_hbm, ct_hbm, rate_ref, gain_ref,
    gin_ref, gw_ref, gfl_ref,
    x_v, wq_v, wf_v, wb_v, wv_v, ct_v,
    a1_s, a1_r, a2_s, a2_r, b1_s, b1_r, b2_s, b2_r,
    w1_s, w1_r, w2_s, w2_r, y_s, rel_r, ysum_s, y_r, fl_s, fl_r,
    in_sem, snd, rcv, y_snd, y_rcv,
):
    me = lax.axis_index("sp")
    tp = lax.axis_index("tp")
    core = lax.rem(me, 2)
    chip = lax.div(me, 2)
    n_chip = n_sp // 2
    tok = x_hbm.shape[0]
    width = x_hbm.shape[1]
    per = n_sp // heads
    my_head = lax.div(me, per)
    q_scale = KDIM ** (-0.5)
    norm_scale = seq_total ** (-0.5)

    loads = [
        pltpu.make_async_copy(src, dst, in_sem.at[i])
        for i, (src, dst) in enumerate(
            [(x_hbm, x_v), (wf_hbm, wf_v), (wb_hbm, wb_v), (wv_hbm, wv_v), (wq_hbm, wq_v), (ct_hbm, ct_v)]
        )
    ]
    for load in loads:
        load.start()
    loading = dict(enumerate(loads))
    flying, sent = {}, []

    def loaded(i):
        loading.pop(i).wait()

    def begun(name, copy):
        flying[name] = copy
        sent.append(copy)

    def arrived(name):
        flying.pop(name).wait_recv()

    def drain():
        for name in list(flying):
            arrived(name)
        for i in list(loading):
            loaded(i)
        for copy in sent:
            copy.wait_send()

    right = (me, lax.rem(tp + 1, n_tp))
    left = (me, lax.rem(tp + n_tp - 1, n_tp))
    barrier = pltpu.get_barrier_semaphore()

    def greet(r, c):
        pl.semaphore_signal(barrier, inc=1, device_id=(lax.rem(me + r, n_sp), tp), device_id_type=MESH)
        return c

    lax.fori_loop(1, n_sp, greet, 0)
    pl.semaphore_signal(barrier, inc=1, device_id=right, device_id_type=MESH)
    pl.semaphore_signal(barrier, inc=1, device_id=left, device_id_type=MESH)

    def put(src, dst, i, device):
        pltpu.make_async_remote_copy(
            src_ref=src, dst_ref=dst, send_sem=snd.at[i], recv_sem=rcv.at[i],
            device_id=device, device_id_type=MESH,
        ).start()

    def took(part, i):
        return pltpu.make_async_remote_copy(
            src_ref=part, dst_ref=part, send_sem=snd.at[i], recv_sem=rcv.at[i],
            device_id=(me, tp), device_id_type=MESH,
        )

    def to_all(source_of, landing, i):
        def step(r, c):
            to = lax.rem(me + r, n_sp)
            put(source_of(to), landing.at[me], i, (to, tp))
            return c

        lax.fori_loop(1, n_sp, step, 0)
        begun(i, took(landing.at[pl.ds(0, n_sp - 1)], i))

    def to_owners(source, landing, i, h):
        mine = lax.rem(me, per)

        def step(r, c):
            to = h * per + lax.rem(mine + r, per)
            put(source.at[to], landing.at[me], i, (to, tp))
            return c

        lax.fori_loop(jnp.where(my_head == h, 1, 0), per, step, 0)
        if h == heads - 1:
            begun(i, took(landing.at[pl.ds(0, n_sp - 1)], i))
            landing[me] = source[me]

    def give_back(result, landing, i):
        def step(r, c):
            to = lax.rem(me + r, n_sp)
            pltpu.make_async_remote_copy(
                src_ref=result.at[to], dst_ref=landing.at[me], send_sem=snd.at[i], recv_sem=rcv.at[i + my_head],
                device_id=(to, tp), device_id_type=MESH,
            ).start()
            return c

        lax.fori_loop(1, n_sp, step, 0)
        sent.append(took(landing.at[pl.ds(0, n_sp - 1)], i))
        landing[me] = result[me]

    def head_arrived(landing, i, h):
        @pl.when(my_head == h)
        def _():
            took(landing.at[pl.ds(h * per, per - 1)], i + h).wait_recv()

        @pl.when(my_head != h)
        def _():
            took(landing.at[pl.ds(h * per, per)], i + h).wait_recv()

    row = lax.broadcasted_iota(jnp.int32, (tok, tok), 0)
    col = lax.broadcasted_iota(jnp.int32, (tok, tok), 1)
    lower = col <= row
    upper = col >= row
    lower_ones = jnp.where(lower, 1.0, 0.0).astype(BF16)
    upper_ones = jnp.where(upper, 1.0, 0.0).astype(BF16)

    loaded(0)
    loaded(1)
    x = x_v[...]
    raw_f = dot(x, wf_v[...], NN).astype(BF16).astype(F32)
    loaded(2)
    raw_b = dot(x, wb_v[...], NN).astype(BF16).astype(F32)
    rate = rate_ref[...] * (1.0 / seq_total)
    key_f, log_f, sp_f, sn_f, open_f = gates(raw_f, rate[0:1])
    key_b, log_b, sp_b, sn_b, open_b = gates(raw_b, rate[1:2])
    cum_f = mm(lower_ones, split(log_f), NN)
    cum_b = mm(upper_ones, split(log_b), NN)
    dec_f = jnp.exp(cum_f[tok - 1 : tok])
    dec_b = jnp.exp(cum_b[0:1])
    head = lambda a, h: a[:, h * KDIM : (h + 1) * KDIM]
    for h in range(heads):
        for p in range(h * per, (h + 1) * per):
            a1_s[p, 16:17, :] = head(dec_f, h)
            a1_s[p, 17:18, :] = head(dec_b, h)

    grow_f, grow_b = jnp.exp(-cum_f), jnp.exp(-cum_b)
    kd_f, kd_b = key_f * grow_f, key_b * grow_b
    kx_f, kx_b = kd_f * dec_f, kd_b * dec_b
    loaded(3)
    v = dot(x, wv_v[...], NN).astype(BF16)
    for h in range(heads):
        kx = split(jnp.concatenate([head(kx_f, h), head(kx_b, h)], axis=1))
        local = mm(head(v, h), kx, TN)
        a1_s[pl.ds(h * per, per), 0:8, :] = local[:, :KDIM].reshape(per, 8, KDIM)
        a1_s[pl.ds(h * per, per), 8:16, :] = local[:, KDIM:].reshape(per, 8, KDIM)

    pl.semaphore_wait(barrier, n_sp + 1)
    for h in range(heads):
        to_owners(a1_s, a1_r, 1, h)

    loaded(4)
    q = dot(x, wq_v[...], NN).astype(BF16).astype(F32) * q_scale
    fade_f, fade_b = jnp.exp(cum_f), jnp.exp(cum_b)
    q_f, q_b = q * fade_f, q * fade_b
    q_fs = [split(head(q_f, h)) for h in range(heads)]
    q_bs = [split(head(q_b, h)) for h in range(heads)]
    kd_fs = [split(head(kd_f, h)) for h in range(heads)]
    kd_bs = [split(head(kd_b, h)) for h in range(heads)]
    scores = []
    inner = []
    for h in range(heads):
        score = jnp.where(lower, mm(q_fs[h], kd_fs[h], NT), 0.0) + jnp.where(upper, mm(q_bs[h], kd_bs[h], NT), 0.0)
        scores.append(split(score))
        inner.append(mm(scores[h], head(v, h), NN))

    def owner_scan(received, result, up_rows, up_dir, down_rows, down_dir):
        up = jnp.zeros((8, KDIM), F32)
        down = jnp.zeros((8, KDIM), F32)
        for j in range(n_sp):
            k = n_sp - 1 - j
            result[j, up_rows, :] = up
            result[k, down_rows, :] = down
            if j < n_sp - 1:
                up = up * a1_r[j, 16 + up_dir : 17 + up_dir, :] + received[j, up_rows, :]
                down = down * a1_r[k, 16 + down_dir : 17 + down_dir, :] + received[k, down_rows, :]

    FWD, BWD = slice(0, 8), slice(8, 16)

    arrived(1)
    owner_scan(a1_r, a2_s, FWD, 0, BWD, 1)
    give_back(a2_s, a2_r, 2)
    loaded(5)
    cot = ct_v[...].astype(F32)
    gain = gain_ref[...]
    def state(buf, h, rows):
        return buf[pl.ds(h * per, per), rows, :].reshape(KDIM, KDIM)

    q_both = [tuple(jnp.concatenate([q_fs[h][i], q_bs[h][i]], axis=1) for i in range(2)) for h in range(heads)]
    both, d_out = [], []
    for h in range(heads):
        head_arrived(a2_r, 2, h)
        both.append(split(jnp.concatenate([state(a2_r, h, FWD), state(a2_r, h, BWD)], axis=1)))
        mixed = inner[h] + mm(q_both[h], both[h], NT)
        inv = lax.rsqrt(jnp.mean(mixed * mixed, axis=-1, keepdims=True) + NORM_EPS)
        scaled = head(cot, h) * gain
        pull = jnp.mean(mixed * scaled, axis=-1, keepdims=True)
        d_mixed = inv * scaled - mixed * (inv * inv * inv * pull)
        d_out.append(split(d_mixed))
        seed = mm(d_out[h], q_both[h], TN)
        b1_s[pl.ds(h * per, per), 0:8, :] = seed[:, :KDIM].reshape(per, 8, KDIM)
        b1_s[pl.ds(h * per, per), 8:16, :] = seed[:, KDIM:].reshape(per, 8, KDIM)
        to_owners(b1_s, b1_r, 4, h)

    dq_f, dq_b, d_low, d_high = [], [], [], []
    for h in range(heads):
        d_score = mm(d_out[h], head(v, h), NT)
        low = split(jnp.where(lower, d_score, 0.0))
        high = split(jnp.where(upper, d_score, 0.0))
        outer = mm(d_out[h], both[h], NN)
        dq_f.append(mm(low, kd_fs[h], NN) + outer[:, :KDIM])
        dq_b.append(mm(high, kd_bs[h], NN) + outer[:, KDIM:])
        d_low.append(low)
        d_high.append(high)
    cat = lambda parts: jnp.concatenate(parts, axis=1)
    g_q = ((cat(dq_f) * fade_f + cat(dq_b) * fade_b) * q_scale).astype(BF16)
    rows_w = width // n_sp
    for i in range(width // KDIM):
        block = dot(x_v[:, i * KDIM : (i + 1) * KDIM], g_q, TN)
        for k in range(KDIM // rows_w):
            p = i * (KDIM // rows_w) + k
            w1_s[p % 2, p // 2] = block[k * rows_w : (k + 1) * rows_w]
    sibling = pltpu.make_async_remote_copy(
        src_ref=w1_s.at[1 - core], dst_ref=w1_r, send_sem=snd.at[7], recv_sem=rcv.at[7],
        device_id=(me + 1 - 2 * core, tp), device_id_type=MESH,
    )
    sibling.start()
    begun(7, sibling)
    dk_f = [mm(d_low[h], q_fs[h], TN) for h in range(heads)]
    dk_b = [mm(d_high[h], q_bs[h], TN) for h in range(heads)]
    dv = [mm(scores[h], d_out[h], TN) for h in range(heads)]
    quarter = width // 4
    rows_y = tok // n_tp
    for c in range(4):
        y_s[c] = dot(g_q, wq_v[c * quarter : (c + 1) * quarter, :], NT).reshape(n_tp, rows_y, quarter)

    arrived(4)
    owner_scan(b1_r, b2_s, BWD, 1, FWD, 0)
    give_back(b2_s, b2_r, 5)

    arrived(7)
    w2_s[...] = w1_s[core] + w1_r[...]

    def to_chip(r, c):
        to = lax.rem(chip + r, n_chip)
        put(w2_s.at[to], w2_r.at[n_chip - r], 8, (to * 2 + core, tp))
        return c

    lax.fori_loop(1, n_chip, to_chip, 0)
    begun(8, took(w2_r.at[pl.ds(1, n_chip - 1)], 8))

    def gate_back(dk, dx, dq, kd, kx, q_d, grow, dec, edge, ones, key, sig_pos, sig_neg, opening):
        along = q_d * dq - kd * dk - kx * dx
        d_log = mm(ones, split(along), NN) + edge
        d_key = grow * (dk + dec * dx) - d_log / (1.0 - key)
        d_raw = -d_key * key * sig_pos
        d_rate = jnp.sum(d_key * sig_neg, axis=0, keepdims=True) * ((1.0 - opening) * (1.0 / seq_total))
        return d_raw.astype(BF16), d_rate

    for h in range(heads):
        head_arrived(b2_r, 5, h)
        back_f, back_b = state(b2_r, h, FWD), state(b2_r, h, BWD)
        back = split(jnp.concatenate([back_f, back_b], axis=1))
        dx = mm(head(v, h), back, NN)
        kx = split(jnp.concatenate([head(kx_f, h), head(kx_b, h)], axis=1))
        g_v = (dv[h] + mm(kx, back, NT)).astype(BF16)
        leave_f = head(dec_f, h) * state(a2_r, h, FWD) + state(a1_s, h, FWD)
        leave_b = head(dec_b, h) * state(a2_r, h, BWD) + state(a1_s, h, BWD)
        edge_f = jnp.sum(leave_f * back_f, axis=0, keepdims=True)
        edge_b = jnp.sum(leave_b * back_b, axis=0, keepdims=True)
        here = lambda *arrays: [head(a, h) for a in arrays]
        g_f, r_f = gate_back(
            dk_f[h], dx[:, :KDIM], dq_f[h], *here(kd_f, kx_f, q_f, grow_f, dec_f), edge_f,
            upper_ones, *here(key_f, sp_f, sn_f, open_f),
        )
        g_b, r_b = gate_back(
            dk_b[h], dx[:, KDIM:], dq_b[h], *here(kd_b, kx_b, q_b, grow_b, dec_b), edge_b,
            lower_ones, *here(key_b, sp_b, sn_b, open_b),
        )
        fl_s[h : h + 1, :] = r_f
        fl_s[heads + h : heads + h + 1, :] = r_b
        mine = slice(h * KDIM, (h + 1) * KDIM)
        for c in range(4):
            rows = slice(c * quarter, (c + 1) * quarter)
            y = (
                dot(g_f, wf_v[rows, mine], NT)
                + dot(g_b, wb_v[rows, mine], NT)
                + dot(g_v, wv_v[rows, mine], NT)
            )
            y_s[c] = y_s[c] + y.reshape(n_tp, rows_y, quarter)

    up, down, across = lax.rem(tp + 1, n_tp), lax.rem(tp + n_tp - 1, n_tp), lax.rem(tp + 2, n_tp)

    def ring(src, dst, i, device):
        return pltpu.make_async_remote_copy(
            src_ref=src, dst_ref=dst, send_sem=y_snd.at[i], recv_sem=y_rcv.at[i],
            device_id=device, device_id_type=MESH,
        )

    relay, direct, summed = [], [], []
    for c in range(4):
        ahead, behind = (right, left) if c % 2 == 0 else (left, right)
        relay.append(ring(y_s.at[c, across], rel_r.at[c], c, ahead))
        direct.append(ring(y_s.at[c, down if c % 2 == 0 else up], y_r.at[c], 4 + c, behind))
        summed.append(ring(ysum_s.at[c], y_r.at[4 + c], 8 + c, ahead))
    for c in range(4):
        relay[c].start()
        begun(("relay", c), relay[c])
    for c in range(4):
        direct[c].start()
        begun(("direct", c), direct[c])
    to_all(lambda to: fl_s, fl_r, 9)
    fl_r[me] = fl_s[...]
    for c in range(4):
        arrived(("relay", c))
        ysum_s[c] = y_s[c, up if c % 2 == 0 else down] + rel_r[c]
        summed[c].start()
        begun(("summed", c), summed[c])

    arrived(9)
    total = fl_r[0]
    for j in range(1, n_sp):
        total = total + fl_r[j]
    total = total * norm_scale
    for h in range(heads):
        gfl_ref[0:1, h * KDIM : (h + 1) * KDIM] = total[h : h + 1]
        gfl_ref[1:2, h * KDIM : (h + 1) * KDIM] = total[heads + h : heads + h + 1]

    arrived(8)
    acc = w2_s[chip]
    for r in range(1, n_chip):
        acc = acc + w2_r[r]
    gw_ref[...] = acc * norm_scale

    for c in range(4):
        arrived(("direct", c))
        arrived(("summed", c))
        gin_ref[:, c * quarter : (c + 1) * quarter] = (y_s[c, tp] + y_r[c] + y_r[4 + c]).astype(BF16)

    drain()


def solution(mesh):
    n_sp, n_tp = mesh.shape["sp"], mesh.shape["tp"]

    def body(block_input, w_query, w_forget_fwd, w_forget_bwd, w_value, floor_rate, gain, cotangent):
        tok, width = block_input.shape
        cols = w_query.shape[1]
        heads = cols // KDIM
        n_chip = n_sp // 2
        rows_w = width // n_sp
        rows_y = tok // n_tp
        quarter = width // 4
        vm = pltpu.VMEM
        pieces = [vm((n_sp, 18 if i < 2 else 16, KDIM), F32) for i in range(8)]
        any_spec = pl.BlockSpec(memory_space=pl.ANY)
        vmem_spec = pl.BlockSpec(memory_space=pltpu.VMEM)
        return pl.pallas_call(
            functools.partial(kernel, n_sp, n_tp, heads, float(tok * n_sp)),
            out_shape=(
                pltpu.VMEM((rows_y, width), BF16),
                pltpu.VMEM((rows_w, cols), F32),
                pltpu.VMEM((2, cols), F32),
            ),
            in_specs=[any_spec] * 6 + [vmem_spec] * 2,
            out_specs=(vmem_spec,) * 3,
            scratch_shapes=[
                vm((tok, width), BF16),
                vm((width, cols), BF16), vm((width, cols), BF16), vm((width, cols), BF16), vm((width, cols), BF16),
                vm((tok, cols), BF16),
                *pieces,
                vm((2, n_chip, rows_w, cols), F32), vm((n_chip, rows_w, cols), F32),
                vm((n_chip, rows_w, cols), F32), vm((n_chip, rows_w, cols), F32),
                vm((4, n_tp, rows_y, quarter), F32), vm((4, rows_y, quarter), F32),
                vm((4, rows_y, quarter), F32), vm((8, rows_y, quarter), F32),
                vm((2 * heads, KDIM), F32), vm((n_sp, 2 * heads, KDIM), F32),
                pltpu.SemaphoreType.DMA((6,)),
                pltpu.SemaphoreType.DMA((10,)),
                pltpu.SemaphoreType.DMA((10,)),
                pltpu.SemaphoreType.DMA((12,)),
                pltpu.SemaphoreType.DMA((12,)),
            ],
            compiler_params=pltpu.CompilerParams(collective_id=0, has_side_effects=True),
        )(block_input, w_query, w_forget_fwd, w_forget_bwd, w_value, cotangent, floor_rate, gain.reshape(1, KDIM))

    return jax.shard_map(
        body,
        mesh=mesh,
        in_specs=(
            P("sp", None), P(None, "tp"), P(None, "tp"), P(None, "tp"), P(None, "tp"), P(None, "tp"), P(), P("sp", "tp"),
        ),
        out_specs=(P(("sp", "tp"), None), P("sp", "tp"), P(None, "tp")),
        check_vma=False,
    )
```

```python
import functools

import jax
import jax.numpy as jnp
from jax import lax
from jax.experimental import pallas as pl
from jax.experimental.pallas import tpu as pltpu
from jax.sharding import PartitionSpec as P

KDIM = 128
NORM_EPS = 1e-06
MESH = pl.DeviceIdType.MESH
F32 = jnp.float32
BF16 = jnp.bfloat16

NN = (((1,), (0,)), ((), ()))
NT = (((1,), (1,)), ((), ()))
TN = (((0,), (0,)), ((), ()))


def dot(a, b, dims):
    return lax.dot_general(a, b, dims, preferred_element_type=F32)


def split(a):
    high = a.astype(BF16)
    return high, (a - high.astype(F32)).astype(BF16)


def mm(a, b, dims):
    if not isinstance(a, tuple):
        return dot(a, b[0], dims) + dot(a, b[1], dims)
    if not isinstance(b, tuple):
        return dot(a[0], b, dims) + dot(a[1], b, dims)
    return dot(a[0], b[0], dims) + (dot(a[1], b[0], dims) + dot(a[0], b[1], dims))


def gates(raw, rate):
    opening = rate * (1.0 - rate * (0.5 - rate * (1.0 / 6.0 - rate * (1.0 / 24.0 - rate * (1.0 / 120.0)))))
    small = jnp.exp(-jnp.abs(raw))
    inverse = 1.0 / (1.0 + small)
    other = small * inverse
    positive = raw >= 0
    sig_pos = jnp.where(positive, inverse, other)
    sig_neg = jnp.where(positive, other, inverse)
    key = opening * sig_neg
    log_forget = -key * (1.0 + key * (0.5 + key * (1.0 / 3.0 + key * (0.25 + key * 0.2))))
    return key, log_forget, sig_pos, sig_neg, opening


def kernel(
    n_sp, n_tp, heads, seq_total,
    x_hbm, wq_hbm, wf_hbm, wb_hbm, wv_hbm, ct_hbm, rate_ref, gain_ref,
    gin_ref, gw_ref, gfl_ref,
    x_v, wq_v, wf_v, wb_v, wv_v, ct_v,
    a1_s, a1_r, a2_s, a2_r, b1_s, b1_r, b2_s, b2_r,
    w1_s, w1_r, w2_s, w2_r, y_s, rel_r, ysum_s, y_r, fl_s, fl_r,
    in_sem, snd, rcv, y_snd, y_rcv,
):
    me = lax.axis_index("sp")
    tp = lax.axis_index("tp")
    core = lax.rem(me, 2)
    chip = lax.div(me, 2)
    n_chip = n_sp // 2
    tok = x_hbm.shape[0]
    width = x_hbm.shape[1]
    per = n_sp // heads
    my_head = lax.div(me, per)
    q_scale = KDIM ** (-0.5)
    norm_scale = seq_total ** (-0.5)

    loads = [
        pltpu.make_async_copy(src, dst, in_sem.at[i])
        for i, (src, dst) in enumerate(
            [(x_hbm, x_v), (wf_hbm, wf_v), (wb_hbm, wb_v), (wv_hbm, wv_v), (wq_hbm, wq_v), (ct_hbm, ct_v)]
        )
    ]
    for load in loads:
        load.start()
    loading = dict(enumerate(loads))
    flying, sent = {}, []

    def loaded(i):
        loading.pop(i).wait()

    def begun(name, copy):
        flying[name] = copy
        sent.append(copy)

    def arrived(name):
        flying.pop(name).wait_recv()

    def drain():
        for name in list(flying):
            arrived(name)
        for i in list(loading):
            loaded(i)
        for copy in sent:
            copy.wait_send()

    right = (me, lax.rem(tp + 1, n_tp))
    left = (me, lax.rem(tp + n_tp - 1, n_tp))
    barrier = pltpu.get_barrier_semaphore()

    def greet(r, c):
        pl.semaphore_signal(barrier, inc=1, device_id=(lax.rem(me + r, n_sp), tp), device_id_type=MESH)
        return c

    lax.fori_loop(1, n_sp, greet, 0)
    pl.semaphore_signal(barrier, inc=1, device_id=right, device_id_type=MESH)
    pl.semaphore_signal(barrier, inc=1, device_id=left, device_id_type=MESH)

    def put(src, dst, i, device):
        pltpu.make_async_remote_copy(
            src_ref=src, dst_ref=dst, send_sem=snd.at[i], recv_sem=rcv.at[i],
            device_id=device, device_id_type=MESH,
        ).start()

    def took(part, i):
        return pltpu.make_async_remote_copy(
            src_ref=part, dst_ref=part, send_sem=snd.at[i], recv_sem=rcv.at[i],
            device_id=(me, tp), device_id_type=MESH,
        )

    def to_all(source_of, landing, i):
        def step(r, c):
            to = lax.rem(me + r, n_sp)
            put(source_of(to), landing.at[me], i, (to, tp))
            return c

        lax.fori_loop(1, n_sp, step, 0)
        begun(i, took(landing.at[pl.ds(0, n_sp - 1)], i))

    def to_owners(source, landing, i, h):
        mine = lax.rem(me, per)

        def step(r, c):
            to = h * per + lax.rem(mine + r, per)
            put(source.at[to], landing.at[me], i, (to, tp))
            return c

        lax.fori_loop(jnp.where(my_head == h, 1, 0), per, step, 0)
        if h == heads - 1:
            begun(i, took(landing.at[pl.ds(0, n_sp - 1)], i))
            landing[me] = source[me]

    def give_back(result, landing, i):
        def step(r, c):
            to = lax.rem(me + r, n_sp)
            pltpu.make_async_remote_copy(
                src_ref=result.at[to], dst_ref=landing.at[me], send_sem=snd.at[i], recv_sem=rcv.at[i + my_head],
                device_id=(to, tp), device_id_type=MESH,
            ).start()
            return c

        lax.fori_loop(1, n_sp, step, 0)
        sent.append(took(landing.at[pl.ds(0, n_sp - 1)], i))
        landing[me] = result[me]

    def head_arrived(landing, i, h):
        @pl.when(my_head == h)
        def _():
            took(landing.at[pl.ds(h * per, per - 1)], i + h).wait_recv()

        @pl.when(my_head != h)
        def _():
            took(landing.at[pl.ds(h * per, per)], i + h).wait_recv()

    row = lax.broadcasted_iota(jnp.int32, (tok, tok), 0)
    col = lax.broadcasted_iota(jnp.int32, (tok, tok), 1)
    lower = col <= row
    upper = col >= row
    lower_ones = jnp.where(lower, 1.0, 0.0).astype(BF16)
    upper_ones = jnp.where(upper, 1.0, 0.0).astype(BF16)

    loaded(0)
    loaded(1)
    x = x_v[...]
    raw_f = dot(x, wf_v[...], NN).astype(BF16).astype(F32)
    loaded(2)
    raw_b = dot(x, wb_v[...], NN).astype(BF16).astype(F32)
    rate = rate_ref[...] * (1.0 / seq_total)
    key_f, log_f, sp_f, sn_f, open_f = gates(raw_f, rate[0:1])
    key_b, log_b, sp_b, sn_b, open_b = gates(raw_b, rate[1:2])
    cum_f = mm(lower_ones, split(log_f), NN)
    cum_b = mm(upper_ones, split(log_b), NN)
    dec_f = jnp.exp(cum_f[tok - 1 : tok])
    dec_b = jnp.exp(cum_b[0:1])
    head = lambda a, h: a[:, h * KDIM : (h + 1) * KDIM]
    for h in range(heads):
        for p in range(h * per, (h + 1) * per):
            a1_s[p, 16:17, :] = head(dec_f, h)
            a1_s[p, 17:18, :] = head(dec_b, h)

    grow_f, grow_b = jnp.exp(-cum_f), jnp.exp(-cum_b)
    kd_f, kd_b = key_f * grow_f, key_b * grow_b
    kx_f, kx_b = kd_f * dec_f, kd_b * dec_b
    loaded(3)
    v = dot(x, wv_v[...], NN).astype(BF16)
    for h in range(heads):
        kx = split(jnp.concatenate([head(kx_f, h), head(kx_b, h)], axis=1))
        local = mm(head(v, h), kx, TN)
        a1_s[pl.ds(h * per, per), 0:8, :] = local[:, :KDIM].reshape(per, 8, KDIM)
        a1_s[pl.ds(h * per, per), 8:16, :] = local[:, KDIM:].reshape(per, 8, KDIM)

    pl.semaphore_wait(barrier, n_sp + 1)
    for h in range(heads):
        to_owners(a1_s, a1_r, 1, h)

    loaded(4)
    q = dot(x, wq_v[...], NN).astype(BF16).astype(F32) * q_scale
    fade_f, fade_b = jnp.exp(cum_f), jnp.exp(cum_b)
    q_f, q_b = q * fade_f, q * fade_b
    q_fs = [split(head(q_f, h)) for h in range(heads)]
    q_bs = [split(head(q_b, h)) for h in range(heads)]
    kd_fs = [split(head(kd_f, h)) for h in range(heads)]
    kd_bs = [split(head(kd_b, h)) for h in range(heads)]
    scores = []
    inner = []
    for h in range(heads):
        score = jnp.where(lower, mm(q_fs[h], kd_fs[h], NT), 0.0) + jnp.where(upper, mm(q_bs[h], kd_bs[h], NT), 0.0)
        scores.append(split(score))
        inner.append(mm(scores[h], head(v, h), NN))

    def owner_scan(received, result, up_rows, up_dir, down_rows, down_dir):
        up = jnp.zeros((8, KDIM), F32)
        down = jnp.zeros((8, KDIM), F32)
        for j in range(n_sp):
            k = n_sp - 1 - j
            result[j, up_rows, :] = up
            result[k, down_rows, :] = down
            if j < n_sp - 1:
                up = up * a1_r[j, 16 + up_dir : 17 + up_dir, :] + received[j, up_rows, :]
                down = down * a1_r[k, 16 + down_dir : 17 + down_dir, :] + received[k, down_rows, :]

    FWD, BWD = slice(0, 8), slice(8, 16)

    arrived(1)
    owner_scan(a1_r, a2_s, FWD, 0, BWD, 1)
    give_back(a2_s, a2_r, 2)
    loaded(5)
    cot = ct_v[...].astype(F32)
    gain = gain_ref[...]
    def state(buf, h, rows):
        return buf[pl.ds(h * per, per), rows, :].reshape(KDIM, KDIM)

    q_both = [tuple(jnp.concatenate([q_fs[h][i], q_bs[h][i]], axis=1) for i in range(2)) for h in range(heads)]
    both, d_out = [], []
    for h in range(heads):
        head_arrived(a2_r, 2, h)
        both.append(split(jnp.concatenate([state(a2_r, h, FWD), state(a2_r, h, BWD)], axis=1)))
        mixed = inner[h] + mm(q_both[h], both[h], NT)
        inv = lax.rsqrt(jnp.mean(mixed * mixed, axis=-1, keepdims=True) + NORM_EPS)
        scaled = head(cot, h) * gain
        pull = jnp.mean(mixed * scaled, axis=-1, keepdims=True)
        d_mixed = inv * scaled - mixed * (inv * inv * inv * pull)
        d_out.append(split(d_mixed))
        seed = mm(d_out[h], q_both[h], TN)
        b1_s[pl.ds(h * per, per), 0:8, :] = seed[:, :KDIM].reshape(per, 8, KDIM)
        b1_s[pl.ds(h * per, per), 8:16, :] = seed[:, KDIM:].reshape(per, 8, KDIM)
        to_owners(b1_s, b1_r, 4, h)

    dq_f, dq_b, d_low, d_high = [], [], [], []
    for h in range(heads):
        d_score = mm(d_out[h], head(v, h), NT)
        low = split(jnp.where(lower, d_score, 0.0))
        high = split(jnp.where(upper, d_score, 0.0))
        outer = mm(d_out[h], both[h], NN)
        dq_f.append(mm(low, kd_fs[h], NN) + outer[:, :KDIM])
        dq_b.append(mm(high, kd_bs[h], NN) + outer[:, KDIM:])
        d_low.append(low)
        d_high.append(high)
    cat = lambda parts: jnp.concatenate(parts, axis=1)
    g_q = ((cat(dq_f) * fade_f + cat(dq_b) * fade_b) * q_scale).astype(BF16)
    rows_w = width // n_sp
    for i in range(width // KDIM):
        block = dot(x_v[:, i * KDIM : (i + 1) * KDIM], g_q, TN)
        for k in range(KDIM // rows_w):
            p = i * (KDIM // rows_w) + k
            w1_s[p % 2, p // 2] = block[k * rows_w : (k + 1) * rows_w]
    sibling = pltpu.make_async_remote_copy(
        src_ref=w1_s.at[1 - core], dst_ref=w1_r, send_sem=snd.at[7], recv_sem=rcv.at[7],
        device_id=(me + 1 - 2 * core, tp), device_id_type=MESH,
    )
    sibling.start()
    begun(7, sibling)
    dk_f = [mm(d_low[h], q_fs[h], TN) for h in range(heads)]
    dk_b = [mm(d_high[h], q_bs[h], TN) for h in range(heads)]
    dv = [mm(scores[h], d_out[h], TN) for h in range(heads)]
    quarter = width // 2
    rows_y = tok // n_tp
    for c in range(2):
        y_s[c] = dot(g_q, wq_v[c * quarter : (c + 1) * quarter, :], NT).reshape(n_tp, rows_y, quarter)

    arrived(4)
    owner_scan(b1_r, b2_s, BWD, 1, FWD, 0)
    give_back(b2_s, b2_r, 5)

    arrived(7)
    w2_s[...] = w1_s[core] + w1_r[...]

    def to_chip(r, c):
        to = lax.rem(chip + r, n_chip)
        put(w2_s.at[to], w2_r.at[n_chip - r], 8, (to * 2 + core, tp))
        return c

    lax.fori_loop(1, n_chip, to_chip, 0)
    begun(8, took(w2_r.at[pl.ds(1, n_chip - 1)], 8))

    def gate_back(dk, dx, dq, kd, kx, q_d, grow, dec, edge, ones, key, sig_pos, sig_neg, opening):
        along = q_d * dq - kd * dk - kx * dx
        d_log = mm(ones, split(along), NN) + edge
        d_key = grow * (dk + dec * dx) - d_log / (1.0 - key)
        d_raw = -d_key * key * sig_pos
        d_rate = jnp.sum(d_key * sig_neg, axis=0, keepdims=True) * ((1.0 - opening) * (1.0 / seq_total))
        return d_raw.astype(BF16), d_rate

    up, down, across = lax.rem(tp + 1, n_tp), lax.rem(tp + n_tp - 1, n_tp), lax.rem(tp + 2, n_tp)

    def ring(src, dst, i, device):
        return pltpu.make_async_remote_copy(
            src_ref=src, dst_ref=dst, send_sem=y_snd.at[i], recv_sem=y_rcv.at[i],
            device_id=device, device_id_type=MESH,
        )

    relay, direct, summed = [], [], []
    for c in range(2):
        ahead, behind = (right, left) if c % 2 == 0 else (left, right)
        relay.append(ring(y_s.at[c, across], rel_r.at[c], c, ahead))
        direct.append(ring(y_s.at[c, down if c % 2 == 0 else up], y_r.at[c], 2 + c, behind))
        summed.append(ring(ysum_s.at[c], y_r.at[2 + c], 4 + c, ahead))
    for h in range(heads):
        head_arrived(b2_r, 5, h)
        back_f, back_b = state(b2_r, h, FWD), state(b2_r, h, BWD)
        back = split(jnp.concatenate([back_f, back_b], axis=1))
        dx = mm(head(v, h), back, NN)
        kx = split(jnp.concatenate([head(kx_f, h), head(kx_b, h)], axis=1))
        g_v = (dv[h] + mm(kx, back, NT)).astype(BF16)
        leave_f = head(dec_f, h) * state(a2_r, h, FWD) + state(a1_s, h, FWD)
        leave_b = head(dec_b, h) * state(a2_r, h, BWD) + state(a1_s, h, BWD)
        edge_f = jnp.sum(leave_f * back_f, axis=0, keepdims=True)
        edge_b = jnp.sum(leave_b * back_b, axis=0, keepdims=True)
        here = lambda *arrays: [head(a, h) for a in arrays]
        g_f, r_f = gate_back(
            dk_f[h], dx[:, :KDIM], dq_f[h], *here(kd_f, kx_f, q_f, grow_f, dec_f), edge_f,
            upper_ones, *here(key_f, sp_f, sn_f, open_f),
        )
        g_b, r_b = gate_back(
            dk_b[h], dx[:, KDIM:], dq_b[h], *here(kd_b, kx_b, q_b, grow_b, dec_b), edge_b,
            lower_ones, *here(key_b, sp_b, sn_b, open_b),
        )
        fl_s[h : h + 1, :] = r_f
        fl_s[heads + h : heads + h + 1, :] = r_b
        mine = slice(h * KDIM, (h + 1) * KDIM)
        for c in range(2):
            rows = slice(c * quarter, (c + 1) * quarter)
            y = (
                dot(g_f, wf_v[rows, mine], NT)
                + dot(g_b, wb_v[rows, mine], NT)
                + dot(g_v, wv_v[rows, mine], NT)
            )
            y_s[c] = y_s[c] + y.reshape(n_tp, rows_y, quarter)
            if h == heads - 1:
                relay[c].start()
                begun(("relay", c), relay[c])

    to_all(lambda to: fl_s, fl_r, 9)
    fl_r[me] = fl_s[...]
    for c in range(2):
        direct[c].start()
        begun(("direct", c), direct[c])
    for c in range(2):
        arrived(("relay", c))
        ysum_s[c] = y_s[c, up if c % 2 == 0 else down] + rel_r[c]
        summed[c].start()
        begun(("summed", c), summed[c])

    arrived(9)
    total = fl_r[0]
    for j in range(1, n_sp):
        total = total + fl_r[j]
    total = total * norm_scale
    for h in range(heads):
        gfl_ref[0:1, h * KDIM : (h + 1) * KDIM] = total[h : h + 1]
        gfl_ref[1:2, h * KDIM : (h + 1) * KDIM] = total[heads + h : heads + h + 1]

    arrived(8)
    acc = w2_s[chip]
    for r in range(1, n_chip):
        acc = acc + w2_r[r]
    gw_ref[...] = acc * norm_scale

    for c in range(2):
        arrived(("direct", c))
        arrived(("summed", c))
        gin_ref[:, c * quarter : (c + 1) * quarter] = (y_s[c, tp] + y_r[c] + y_r[2 + c]).astype(BF16)

    drain()


def solution(mesh):
    n_sp, n_tp = mesh.shape["sp"], mesh.shape["tp"]

    def body(block_input, w_query, w_forget_fwd, w_forget_bwd, w_value, floor_rate, gain, cotangent):
        tok, width = block_input.shape
        cols = w_query.shape[1]
        heads = cols // KDIM
        n_chip = n_sp // 2
        rows_w = width // n_sp
        rows_y = tok // n_tp
        quarter = width // 2
        vm = pltpu.VMEM
        pieces = [vm((n_sp, 18 if i < 2 else 16, KDIM), F32) for i in range(8)]
        any_spec = pl.BlockSpec(memory_space=pl.ANY)
        vmem_spec = pl.BlockSpec(memory_space=pltpu.VMEM)
        return pl.pallas_call(
            functools.partial(kernel, n_sp, n_tp, heads, float(tok * n_sp)),
            out_shape=(
                pltpu.VMEM((rows_y, width), BF16),
                pltpu.VMEM((rows_w, cols), F32),
                pltpu.VMEM((2, cols), F32),
            ),
            in_specs=[any_spec] * 6 + [vmem_spec] * 2,
            out_specs=(vmem_spec,) * 3,
            scratch_shapes=[
                vm((tok, width), BF16),
                vm((width, cols), BF16), vm((width, cols), BF16), vm((width, cols), BF16), vm((width, cols), BF16),
                vm((tok, cols), BF16),
                *pieces,
                vm((2, n_chip, rows_w, cols), F32), vm((n_chip, rows_w, cols), F32),
                vm((n_chip, rows_w, cols), F32), vm((n_chip, rows_w, cols), F32),
                vm((2, n_tp, rows_y, quarter), F32), vm((4, rows_y, quarter), F32),
                vm((4, rows_y, quarter), F32), vm((8, rows_y, quarter), F32),
                vm((2 * heads, KDIM), F32), vm((n_sp, 2 * heads, KDIM), F32),
                pltpu.SemaphoreType.DMA((6,)),
                pltpu.SemaphoreType.DMA((10,)),
                pltpu.SemaphoreType.DMA((10,)),
                pltpu.SemaphoreType.DMA((12,)),
                pltpu.SemaphoreType.DMA((12,)),
            ],
            compiler_params=pltpu.CompilerParams(collective_id=0, has_side_effects=True),
        )(block_input, w_query, w_forget_fwd, w_forget_bwd, w_value, cotangent, floor_rate, gain.reshape(1, KDIM))

    return jax.shard_map(
        body,
        mesh=mesh,
        in_specs=(
            P("sp", None), P(None, "tp"), P(None, "tp"), P(None, "tp"), P(None, "tp"), P(None, "tp"), P(), P("sp", "tp"),
        ),
        out_specs=(P(("sp", "tp"), None), P("sp", "tp"), P(None, "tp")),
        check_vma=False,
    )
```

```python
import functools

import jax
import jax.numpy as jnp
from jax import lax
from jax.experimental import pallas as pl
from jax.experimental.pallas import tpu as pltpu
from jax.sharding import PartitionSpec as P

KDIM = 128
NORM_EPS = 1e-06
MESH = pl.DeviceIdType.MESH
F32 = jnp.float32
BF16 = jnp.bfloat16

NN = (((1,), (0,)), ((), ()))
NT = (((1,), (1,)), ((), ()))
TN = (((0,), (0,)), ((), ()))


def dot(a, b, dims):
    return lax.dot_general(a, b, dims, preferred_element_type=F32)


def split(a):
    high = a.astype(BF16)
    return high, (a - high.astype(F32)).astype(BF16)


def mm(a, b, dims):
    if not isinstance(a, tuple):
        return dot(a, b[0], dims) + dot(a, b[1], dims)
    if not isinstance(b, tuple):
        return dot(a[0], b, dims) + dot(a[1], b, dims)
    return dot(a[0], b[0], dims) + (dot(a[1], b[0], dims) + dot(a[0], b[1], dims))


def gates(raw, rate):
    opening = rate * (1.0 - rate * (0.5 - rate * (1.0 / 6.0 - rate * (1.0 / 24.0 - rate * (1.0 / 120.0)))))
    small = jnp.exp(-jnp.abs(raw))
    inverse = 1.0 / (1.0 + small)
    other = small * inverse
    positive = raw >= 0
    sig_pos = jnp.where(positive, inverse, other)
    sig_neg = jnp.where(positive, other, inverse)
    key = opening * sig_neg
    log_forget = -key * (1.0 + key * (0.5 + key * (1.0 / 3.0 + key * (0.25 + key * 0.2))))
    return key, log_forget, sig_pos, sig_neg, opening


def kernel(
    n_sp, n_tp, heads, seq_total,
    x_hbm, wq_hbm, wf_hbm, wb_hbm, wv_hbm, ct_hbm, rate_ref, gain_ref,
    gin_ref, gw_ref, gfl_ref,
    x_v, wq_v, wf_v, wb_v, wv_v, ct_v,
    a1_s, a1_r, a2_s, a2_r, b1_s, b1_r, b2_s, b2_r,
    w1_s, w1_r, w2_s, w2_r, y_s, rel_r, ysum_s, y_r, fl_s, fl_r,
    in_sem, snd, rcv, y_snd, y_rcv,
):
    me = lax.axis_index("sp")
    tp = lax.axis_index("tp")
    core = lax.rem(me, 2)
    chip = lax.div(me, 2)
    n_chip = n_sp // 2
    tok = x_hbm.shape[0]
    width = x_hbm.shape[1]
    per = n_sp // heads
    my_head = lax.div(me, per)
    q_scale = KDIM ** (-0.5)
    norm_scale = seq_total ** (-0.5)

    loads = [
        pltpu.make_async_copy(src, dst, in_sem.at[i])
        for i, (src, dst) in enumerate(
            [(x_hbm, x_v), (wf_hbm, wf_v), (wb_hbm, wb_v), (wv_hbm, wv_v), (wq_hbm, wq_v), (ct_hbm, ct_v)]
        )
    ]
    for load in loads:
        load.start()
    loading = dict(enumerate(loads))
    flying, sent = {}, []

    def loaded(i):
        loading.pop(i).wait()

    def begun(name, copy):
        flying[name] = copy
        sent.append(copy)

    def arrived(name):
        flying.pop(name).wait_recv()

    def drain():
        for name in list(flying):
            arrived(name)
        for i in list(loading):
            loaded(i)
        for copy in sent:
            copy.wait_send()

    right = (me, lax.rem(tp + 1, n_tp))
    left = (me, lax.rem(tp + n_tp - 1, n_tp))
    barrier = pltpu.get_barrier_semaphore()

    def greet(r, c):
        pl.semaphore_signal(barrier, inc=1, device_id=(lax.rem(me + r, n_sp), tp), device_id_type=MESH)
        return c

    lax.fori_loop(1, n_sp, greet, 0)
    pl.semaphore_signal(barrier, inc=1, device_id=right, device_id_type=MESH)
    pl.semaphore_signal(barrier, inc=1, device_id=left, device_id_type=MESH)

    def put(src, dst, i, device):
        pltpu.make_async_remote_copy(
            src_ref=src, dst_ref=dst, send_sem=snd.at[i], recv_sem=rcv.at[i],
            device_id=device, device_id_type=MESH,
        ).start()

    def took(part, i):
        return pltpu.make_async_remote_copy(
            src_ref=part, dst_ref=part, send_sem=snd.at[i], recv_sem=rcv.at[i],
            device_id=(me, tp), device_id_type=MESH,
        )

    def to_all(source_of, landing, i):
        def step(r, c):
            to = lax.rem(me + r, n_sp)
            put(source_of(to), landing.at[me], i, (to, tp))
            return c

        lax.fori_loop(1, n_sp, step, 0)
        begun(i, took(landing.at[pl.ds(0, n_sp - 1)], i))

    def to_owners(source, landing, i, h):
        mine = lax.rem(me, per)

        def step(r, c):
            to = h * per + lax.rem(mine + r, per)
            put(source.at[to], landing.at[me], i, (to, tp))
            return c

        lax.fori_loop(jnp.where(my_head == h, 1, 0), per, step, 0)
        if h == heads - 1:
            begun(i, took(landing.at[pl.ds(0, n_sp - 1)], i))
            landing[me] = source[me]

    def give_back(result, landing, i):
        def step(r, c):
            to = lax.rem(me + r, n_sp)
            pltpu.make_async_remote_copy(
                src_ref=result.at[to], dst_ref=landing.at[me], send_sem=snd.at[i], recv_sem=rcv.at[i + my_head],
                device_id=(to, tp), device_id_type=MESH,
            ).start()
            return c

        lax.fori_loop(1, n_sp, step, 0)
        sent.append(took(landing.at[pl.ds(0, n_sp - 1)], i))
        landing[me] = result[me]

    def head_arrived(landing, i, h):
        @pl.when(my_head == h)
        def _():
            took(landing.at[pl.ds(h * per, per - 1)], i + h).wait_recv()

        @pl.when(my_head != h)
        def _():
            took(landing.at[pl.ds(h * per, per)], i + h).wait_recv()

    row = lax.broadcasted_iota(jnp.int32, (tok, tok), 0)
    col = lax.broadcasted_iota(jnp.int32, (tok, tok), 1)
    lower = col <= row
    upper = col >= row
    lower_ones = jnp.where(lower, 1.0, 0.0).astype(BF16)
    upper_ones = jnp.where(upper, 1.0, 0.0).astype(BF16)

    loaded(0)
    loaded(1)
    x = x_v[...]
    raw_f = dot(x, wf_v[...], NN).astype(BF16).astype(F32)
    loaded(2)
    raw_b = dot(x, wb_v[...], NN).astype(BF16).astype(F32)
    rate = rate_ref[...] * (1.0 / seq_total)
    key_f, log_f, sp_f, sn_f, open_f = gates(raw_f, rate[0:1])
    key_b, log_b, sp_b, sn_b, open_b = gates(raw_b, rate[1:2])
    cum_f = mm(lower_ones, split(log_f), NN)
    cum_b = mm(upper_ones, split(log_b), NN)
    dec_f = jnp.exp(cum_f[tok - 1 : tok])
    dec_b = jnp.exp(cum_b[0:1])
    head = lambda a, h: a[:, h * KDIM : (h + 1) * KDIM]
    for h in range(heads):
        for p in range(h * per, (h + 1) * per):
            a1_s[p, 16:17, :] = head(dec_f, h)
            a1_s[p, 17:18, :] = head(dec_b, h)

    grow_f, grow_b = jnp.exp(-cum_f), jnp.exp(-cum_b)
    kd_f, kd_b = key_f * grow_f, key_b * grow_b
    kx_f, kx_b = kd_f * dec_f, kd_b * dec_b
    loaded(3)
    v = dot(x, wv_v[...], NN).astype(BF16)
    for h in range(heads):
        kx = split(jnp.concatenate([head(kx_f, h), head(kx_b, h)], axis=1))
        local = mm(head(v, h), kx, TN)
        a1_s[pl.ds(h * per, per), 0:8, :] = local[:, :KDIM].reshape(per, 8, KDIM)
        a1_s[pl.ds(h * per, per), 8:16, :] = local[:, KDIM:].reshape(per, 8, KDIM)

    pl.semaphore_wait(barrier, n_sp + 1)
    for h in range(heads):
        to_owners(a1_s, a1_r, 1, h)

    loaded(4)
    q = dot(x, wq_v[...], NN).astype(BF16).astype(F32) * q_scale
    fade_f, fade_b = jnp.exp(cum_f), jnp.exp(cum_b)
    q_f, q_b = q * fade_f, q * fade_b
    q_fs = [split(head(q_f, h)) for h in range(heads)]
    q_bs = [split(head(q_b, h)) for h in range(heads)]
    kd_fs = [split(head(kd_f, h)) for h in range(heads)]
    kd_bs = [split(head(kd_b, h)) for h in range(heads)]
    scores = []
    inner = []
    for h in range(heads):
        score = jnp.where(lower, mm(q_fs[h], kd_fs[h], NT), 0.0) + jnp.where(upper, mm(q_bs[h], kd_bs[h], NT), 0.0)
        scores.append(split(score))
        inner.append(mm(scores[h], head(v, h), NN))

    def owner_scan(received, result, up_rows, up_dir, down_rows, down_dir):
        up = jnp.zeros((8, KDIM), F32)
        down = jnp.zeros((8, KDIM), F32)
        for j in range(n_sp):
            k = n_sp - 1 - j
            result[j, up_rows, :] = up
            result[k, down_rows, :] = down
            if j < n_sp - 1:
                up = up * a1_r[j, 16 + up_dir : 17 + up_dir, :] + received[j, up_rows, :]
                down = down * a1_r[k, 16 + down_dir : 17 + down_dir, :] + received[k, down_rows, :]

    FWD, BWD = slice(0, 8), slice(8, 16)

    arrived(1)
    owner_scan(a1_r, a2_s, FWD, 0, BWD, 1)
    give_back(a2_s, a2_r, 2)
    loaded(5)
    cot = ct_v[...].astype(F32)
    gain = gain_ref[...]
    def state(buf, h, rows):
        return buf[pl.ds(h * per, per), rows, :].reshape(KDIM, KDIM)

    q_both = [tuple(jnp.concatenate([q_fs[h][i], q_bs[h][i]], axis=1) for i in range(2)) for h in range(heads)]
    both, d_out = [], []
    for h in range(heads):
        head_arrived(a2_r, 2, h)
        both.append(split(jnp.concatenate([state(a2_r, h, FWD), state(a2_r, h, BWD)], axis=1)))
        mixed = inner[h] + mm(q_both[h], both[h], NT)
        inv = lax.rsqrt(jnp.mean(mixed * mixed, axis=-1, keepdims=True) + NORM_EPS)
        scaled = head(cot, h) * gain
        pull = jnp.mean(mixed * scaled, axis=-1, keepdims=True)
        d_mixed = inv * scaled - mixed * (inv * inv * inv * pull)
        d_out.append(split(d_mixed))
        seed = mm(d_out[h], q_both[h], TN)
        b1_s[pl.ds(h * per, per), 0:8, :] = seed[:, :KDIM].reshape(per, 8, KDIM)
        b1_s[pl.ds(h * per, per), 8:16, :] = seed[:, KDIM:].reshape(per, 8, KDIM)
        to_owners(b1_s, b1_r, 4, h)

    dq_f, dq_b, d_low, d_high = [], [], [], []
    for h in range(heads):
        d_score = mm(d_out[h], head(v, h), NT)
        low = split(jnp.where(lower, d_score, 0.0))
        high = split(jnp.where(upper, d_score, 0.0))
        outer = mm(d_out[h], both[h], NN)
        dq_f.append(mm(low, kd_fs[h], NN) + outer[:, :KDIM])
        dq_b.append(mm(high, kd_bs[h], NN) + outer[:, KDIM:])
        d_low.append(low)
        d_high.append(high)
    cat = lambda parts: jnp.concatenate(parts, axis=1)
    g_q = ((cat(dq_f) * fade_f + cat(dq_b) * fade_b) * q_scale).astype(BF16)
    rows_w = width // n_sp
    for i in range(width // KDIM):
        block = dot(x_v[:, i * KDIM : (i + 1) * KDIM], g_q, TN)
        for k in range(KDIM // rows_w):
            p = i * (KDIM // rows_w) + k
            w1_s[p % 2, p // 2] = block[k * rows_w : (k + 1) * rows_w]
    sibling = pltpu.make_async_remote_copy(
        src_ref=w1_s.at[1 - core], dst_ref=w1_r, send_sem=snd.at[7], recv_sem=rcv.at[7],
        device_id=(me + 1 - 2 * core, tp), device_id_type=MESH,
    )
    sibling.start()
    begun(7, sibling)
    dk_f = [mm(d_low[h], q_fs[h], TN) for h in range(heads)]
    dk_b = [mm(d_high[h], q_bs[h], TN) for h in range(heads)]
    dv = [mm(scores[h], d_out[h], TN) for h in range(heads)]
    quarter = width // 4
    rows_y = tok // n_tp
    for c in range(4):
        y_s[c] = dot(g_q, wq_v[c * quarter : (c + 1) * quarter, :], NT).reshape(n_tp, rows_y, quarter)

    arrived(4)
    owner_scan(b1_r, b2_s, BWD, 1, FWD, 0)
    give_back(b2_s, b2_r, 5)

    arrived(7)
    w2_s[...] = w1_s[core] + w1_r[...]

    def to_chip(r, c):
        to = lax.rem(chip + r, n_chip)
        put(w2_s.at[to], w2_r.at[n_chip - r], 8, (to * 2 + core, tp))
        return c

    lax.fori_loop(1, n_chip, to_chip, 0)
    begun(8, took(w2_r.at[pl.ds(1, n_chip - 1)], 8))

    def gate_back(dk, dx, dq, kd, kx, q_d, grow, dec, edge, ones, key, sig_pos, sig_neg, opening):
        along = q_d * dq - kd * dk - kx * dx
        d_log = mm(ones, split(along), NN) + edge
        d_key = grow * (dk + dec * dx) - d_log / (1.0 - key)
        d_raw = -d_key * key * sig_pos
        d_rate = jnp.sum(d_key * sig_neg, axis=0, keepdims=True) * ((1.0 - opening) * (1.0 / seq_total))
        return d_raw.astype(BF16), d_rate

    for h in range(heads):
        head_arrived(b2_r, 5, h)
        back_f, back_b = state(b2_r, h, FWD), state(b2_r, h, BWD)
        back = split(jnp.concatenate([back_f, back_b], axis=1))
        dx = mm(head(v, h), back, NN)
        kx = split(jnp.concatenate([head(kx_f, h), head(kx_b, h)], axis=1))
        g_v = (dv[h] + mm(kx, back, NT)).astype(BF16)
        leave_f = head(dec_f, h) * state(a2_r, h, FWD) + state(a1_s, h, FWD)
        leave_b = head(dec_b, h) * state(a2_r, h, BWD) + state(a1_s, h, BWD)
        edge_f = jnp.sum(leave_f * back_f, axis=0, keepdims=True)
        edge_b = jnp.sum(leave_b * back_b, axis=0, keepdims=True)
        here = lambda *arrays: [head(a, h) for a in arrays]
        g_f, r_f = gate_back(
            dk_f[h], dx[:, :KDIM], dq_f[h], *here(kd_f, kx_f, q_f, grow_f, dec_f), edge_f,
            upper_ones, *here(key_f, sp_f, sn_f, open_f),
        )
        g_b, r_b = gate_back(
            dk_b[h], dx[:, KDIM:], dq_b[h], *here(kd_b, kx_b, q_b, grow_b, dec_b), edge_b,
            lower_ones, *here(key_b, sp_b, sn_b, open_b),
        )
        fl_s[h : h + 1, :] = r_f
        fl_s[heads + h : heads + h + 1, :] = r_b
        mine = slice(h * KDIM, (h + 1) * KDIM)
        for c in range(4):
            rows = slice(c * quarter, (c + 1) * quarter)
            y = (
                dot(g_f, wf_v[rows, mine], NT)
                + dot(g_b, wb_v[rows, mine], NT)
                + dot(g_v, wv_v[rows, mine], NT)
            )
            y_s[c] = y_s[c] + y.reshape(n_tp, rows_y, quarter)

    up, down, across = lax.rem(tp + 1, n_tp), lax.rem(tp + n_tp - 1, n_tp), lax.rem(tp + 2, n_tp)

    def ring(src, dst, i, device):
        return pltpu.make_async_remote_copy(
            src_ref=src, dst_ref=dst, send_sem=y_snd.at[i], recv_sem=y_rcv.at[i],
            device_id=device, device_id_type=MESH,
        )

    relay, direct, summed = [], [], []
    for c in range(4):
        ahead, behind = (right, left) if c % 2 == 0 else (left, right)
        relay.append(ring(y_s.at[c, across], rel_r.at[c], c, ahead))
        direct.append(ring(y_s.at[c, down if c % 2 == 0 else up], y_r.at[c], 4 + c, behind))
        summed.append(ring(ysum_s.at[c], y_r.at[4 + c], 8 + c, ahead))
    for c in range(4):
        relay[c].start()
        begun(("relay", c), relay[c])
    to_all(lambda to: fl_s, fl_r, 9)
    fl_r[me] = fl_s[...]
    for c in range(4):
        direct[c].start()
        begun(("direct", c), direct[c])
    for c in range(4):
        arrived(("relay", c))
        ysum_s[c] = y_s[c, up if c % 2 == 0 else down] + rel_r[c]
        summed[c].start()
        begun(("summed", c), summed[c])

    arrived(9)
    total = fl_r[0]
    for j in range(1, n_sp):
        total = total + fl_r[j]
    total = total * norm_scale
    for h in range(heads):
        gfl_ref[0:1, h * KDIM : (h + 1) * KDIM] = total[h : h + 1]
        gfl_ref[1:2, h * KDIM : (h + 1) * KDIM] = total[heads + h : heads + h + 1]

    arrived(8)
    acc = w2_s[chip]
    for r in range(1, n_chip):
        acc = acc + w2_r[r]
    gw_ref[...] = acc * norm_scale

    for c in range(4):
        arrived(("direct", c))
        arrived(("summed", c))
        gin_ref[:, c * quarter : (c + 1) * quarter] = (y_s[c, tp] + y_r[c] + y_r[4 + c]).astype(BF16)

    drain()


def solution(mesh):
    n_sp, n_tp = mesh.shape["sp"], mesh.shape["tp"]

    def body(block_input, w_query, w_forget_fwd, w_forget_bwd, w_value, floor_rate, gain, cotangent):
        tok, width = block_input.shape
        cols = w_query.shape[1]
        heads = cols // KDIM
        n_chip = n_sp // 2
        rows_w = width // n_sp
        rows_y = tok // n_tp
        quarter = width // 4
        vm = pltpu.VMEM
        pieces = [vm((n_sp, 18 if i < 2 else 16, KDIM), F32) for i in range(8)]
        any_spec = pl.BlockSpec(memory_space=pl.ANY)
        vmem_spec = pl.BlockSpec(memory_space=pltpu.VMEM)
        return pl.pallas_call(
            functools.partial(kernel, n_sp, n_tp, heads, float(tok * n_sp)),
            out_shape=(
                pltpu.VMEM((rows_y, width), BF16),
                pltpu.VMEM((rows_w, cols), F32),
                pltpu.VMEM((2, cols), F32),
            ),
            in_specs=[any_spec] * 6 + [vmem_spec] * 2,
            out_specs=(vmem_spec,) * 3,
            scratch_shapes=[
                vm((tok, width), BF16),
                vm((width, cols), BF16), vm((width, cols), BF16), vm((width, cols), BF16), vm((width, cols), BF16),
                vm((tok, cols), BF16),
                *pieces,
                vm((2, n_chip, rows_w, cols), F32), vm((n_chip, rows_w, cols), F32),
                vm((n_chip, rows_w, cols), F32), vm((n_chip, rows_w, cols), F32),
                vm((4, n_tp, rows_y, quarter), F32), vm((4, rows_y, quarter), F32),
                vm((4, rows_y, quarter), F32), vm((8, rows_y, quarter), F32),
                vm((2 * heads, KDIM), F32), vm((n_sp, 2 * heads, KDIM), F32),
                pltpu.SemaphoreType.DMA((6,)),
                pltpu.SemaphoreType.DMA((10,)),
                pltpu.SemaphoreType.DMA((10,)),
                pltpu.SemaphoreType.DMA((12,)),
                pltpu.SemaphoreType.DMA((12,)),
            ],
            compiler_params=pltpu.CompilerParams(collective_id=0, has_side_effects=True),
        )(block_input, w_query, w_forget_fwd, w_forget_bwd, w_value, cotangent, floor_rate, gain.reshape(1, KDIM))

    return jax.shard_map(
        body,
        mesh=mesh,
        in_specs=(
            P("sp", None), P(None, "tp"), P(None, "tp"), P(None, "tp"), P(None, "tp"), P(None, "tp"), P(), P("sp", "tp"),
        ),
        out_specs=(P(("sp", "tp"), None), P("sp", "tp"), P(None, "tp")),
        check_vma=False,
    )
```
